32 devices in a mesh: ep: 8 (over z, core), tp: 4 (over y, x).
Axes of the slice: x: 2, y: 2, z: 4, core: 2. Of those that a mesh axis runs over, the one named last changes fastest.
Arguments:
- tokens: bfloat16 [256, 2048], P('ep'), may hold values from -6 to 6
- recurrent_head_state: float32 [256, 16, 4096], P('ep', 'tp'), may hold values from -4 to 4
- first_norm_gain: float32 [2048], replicated, may hold values from 0.1 to 1.9
- receptance_matrix: bfloat16 [2048, 1024], P(None, 'tp'), may hold values from -0.125 to 0.125
- key_matrix: bfloat16 [2048, 1024], P(None, 'tp'), may hold values from -0.125 to 0.125
- value_matrix: bfloat16 [2048, 1024], P(None, 'tp'), may hold values from -0.125 to 0.125
- decay_matrix: bfloat16 [2048, 1024], P(None, 'tp'), may hold values from -0.125 to 0.125
- decay_offset: float32 [1024], P('tp'), may hold values from -3 to 0.5
- correction_offset: float32 [1024], P('tp'), may hold values from -2 to 2
- correction_key_factor: float32 [1024], P('tp'), may hold values from -1 to 1
- own_term_weight: float32 [1024], P('tp'), may hold values from -0.9 to 0.9
- head_norm_gain: float32 [1024], P('tp'), may hold values from 0.1 to 1.9
- output_matrix: bfloat16 [1024, 2048], P('tp'), may hold values from -0.1875 to 0.1875
- second_norm_gain: float32 [2048], replicated, may hold values from 0.1 to 1.9
- routing: int32 [256, 2], replicated, may hold values from 0 to 7, all different within a row; in each aligned block of 32 rows (0 to 31, 32 to 63, ...) at most 16 rows name the same one
- routing_weight: float32 [256, 2], P('ep'), may hold values from 0.1 to 1
- expert_gate_weight: bfloat16 [8, 2048, 4096], P('ep', None, 'tp'), may hold values from -0.125 to 0.125
- expert_up_weight: bfloat16 [8, 2048, 4096], P('ep', None, 'tp'), may hold values from -0.125 to 0.125
- expert_down_weight: bfloat16 [8, 4096, 2048], P('ep', 'tp'), may hold values from -0.125 to 0.125
- dense_gate_weight: bfloat16 [2048, 2816], P(None, 'ep'), may hold values from -0.125 to 0.125
- dense_up_weight: bfloat16 [2048, 2816], P(None, 'ep'), may hold values from -0.125 to 0.125
- dense_down_weight: bfloat16 [2816, 2048], P('ep'), may hold values from -0.109375 to 0.109375
- dense_gate_offset: float32 [2048], replicated, may hold values from -3 to 3
Outputs:
- layer_out: bfloat16 [256, 2048], P(('ep', 'tp'))
- next_state: float32 [256, 16, 4096], P('ep', 'tp')
The draws below stay inside these ranges and needn't reach their ends.
Inputs may be any that keep to these rules, and one draw needn't show every extreme that they name: `routing`: each row names 2 different experts. In each aligned block of 32 rows no expert is named more than 16 times, a bound that some block reaches.
All inputs are finite; a program needn't handle non-finite values.
Results may differ from the reference program's by a relative error of at most 0.017.
Values may be sent and summed in bfloat16 or wider, within the bound.
A program may use at most 64 MiB of HBM per device.

```python
import math
from functools import partial
import jax
import jax.numpy as jnp
import numpy as np
from jax import lax

D = 2048
HEAD_COUNT = 16
HEAD_WIDTH = 64
FF_E = 4096
FF_D = 2816
TOP_K = 2
B_DEV = 32
B_TOT = 256
EXPERTS = 8
CAP = 16
N_EP = 8


def strengthened(entries, rng, source, target, parts, factor):
    def block_of(axis_at):
        return (jnp.arange(entries.shape[axis_at]) // (entries.shape[axis_at] // parts)).reshape((-1,) + (1,) * (entries.ndim - 1 - axis_at))

    first = jax.random.permutation(rng, parts)[block_of(target)]
    second = (block_of(target) + parts // 2) % parts
    return jnp.where((block_of(source) == first) | (block_of(source) == second), factor * entries, entries)


def levels(rng, extent, pieces, smallest, high):
    level, own = 1.0, jax.random.fold_in(rng, 6)
    for position, blocks in pieces:
        draws = jnp.exp(jax.random.uniform(jax.random.fold_in(own, position), (blocks,), jnp.float32, smallest / len(pieces), high / len(pieces)))
        level = level * jnp.repeat(draws, extent[position] // blocks).reshape([-1 if axis == position else 1 for axis in range(len(extent))])
    return level


def shared_out(stream_key, own, number, rows, amount, top, most, lean):
    sequence = jax.random.permutation(stream_key, amount)
    crowded, common = shares(amount, rows * top, most, lean, True), shares(amount, rows * top, most, lean, False)
    places = jnp.arange(amount)

    def named(tallies, turn):
        used = int((tallies > 0).sum())
        fixed = max(1, used // 4)
        moved = fixed + (places - fixed + turn * (used - fixed)) % max(1, amount - fixed)
        return jnp.zeros((amount,), jnp.int32).at[sequence[jnp.where(places < fixed, places, moved)]].set(jnp.asarray(tallies, jnp.int32))

    tallies = jnp.where(number % 4 == 0, named(crowded, number // 4), named(common, number - number // 4 - 1))
    mixed = jax.random.permutation(jax.random.fold_in(own, 3), amount)
    giver, receiver = mixed[0:amount // 2 * 2:2], mixed[1:amount // 2 * 2:2]
    room = jnp.minimum(tallies[giver] - 1, most - tallies[receiver]) // 2
    room = jnp.where((giver == sequence[0]) | (receiver == sequence[0]) | (tallies[receiver] == 0), 0, jnp.maximum(room, 0))
    moved = jax.random.randint(jax.random.fold_in(own, 4), (amount // 2,), 0, 1 << 20) % (room + 1)
    tallies = tallies.at[giver].add(-moved).at[receiver].add(moved)
    labels = jnp.searchsorted(jnp.cumsum(tallies), jnp.arange(rows * top), side="right").astype(jnp.int32)
    listing = labels.reshape(top, rows).T
    listing = listing[jax.random.permutation(jax.random.fold_in(own, 1), rows)]
    turn = jax.random.randint(jax.random.fold_in(own, 2), (rows, 1), 0, top)
    return jnp.take_along_axis(listing, (jnp.arange(top)[None, :] + turn) % top, axis=1)


def shares(amount, total, reach, slope, full):
    weights = [(1 << 20) // math.isqrt(grade ** slope) + 1 for grade in range(1, amount + 1)]
    largest = reach if full else min(reach, max(-(-total // amount), total * weights[0] // sum(weights)))
    least = 1 if total - largest >= amount - 1 else 0
    counts, spare = [largest] + [least] * (amount - 1), total - largest - least * (amount - 1)
    while spare > 0:
        movable = [i for i in range(1, amount) if counts[i] < largest] or [i for i in range(1, amount) if counts[i] < reach]
        pool, left = sum([weights[i] for i in movable]), spare
        for i in movable:
            extra = min(reach - counts[i], max(1, left * weights[i] // pool), spare)
            counts[i] = counts[i] + extra
            spare = spare - extra
    return np.array(counts)


def bell_draw(stream_key, dims, width, limit, split=(), kind=jnp.bfloat16):
    entries = jax.random.normal(stream_key, dims, jnp.float32) * width
    if len(split) > 0:
        entries = levels(stream_key, dims, split, -0.22, 0.18) * entries
    return jnp.clip(entries, min=-limit, max=limit).astype(kind)


def gaussian_with(rng, dims, scale, limit, pieces, heavy, kind=jnp.bfloat16):
    drawn = scale * jax.random.normal(rng, dims, jnp.float32)
    if pieces:
        drawn = drawn * levels(rng, dims, pieces, -0.22, 0.18)
    return jnp.clip(strengthened(drawn, jax.random.fold_in(rng, 3), *heavy), -limit, limit).astype(kind)


def setup_inputs(seed: int = 0) -> dict:
    streams_of = jax.random.split(jax.random.key(seed), 24)
    tokens = bell_draw(streams_of[0], (B_TOT, D), 1.0, 6.0, ((0, 8),))
    recurrent_head_state = bell_draw(streams_of[1], (B_TOT, HEAD_COUNT, HEAD_WIDTH * HEAD_WIDTH), 0.5, 4.0, ((0, 8), (1, 4)), jnp.float32)
    first_norm_gain = jnp.clip(1.0 + 0.18 * jax.random.normal(streams_of[2], (D,), jnp.float32), 0.1, 1.9)
    receptance_matrix = bell_draw(streams_of[3], (D, HEAD_COUNT * HEAD_WIDTH), D ** -0.5, 0.125, ((1, 4),))
    key_matrix = bell_draw(streams_of[4], (D, HEAD_COUNT * HEAD_WIDTH), D ** -0.5, 0.125, ((1, 4),))
    value_matrix = bell_draw(streams_of[5], (D, HEAD_COUNT * HEAD_WIDTH), D ** -0.5, 0.125, ((1, 4),))
    decay_matrix = bell_draw(streams_of[6], (D, HEAD_COUNT * HEAD_WIDTH), D ** -0.5, 0.125, ((1, 4),))
    decay_offset = jnp.clip(-3.0 + 3.5 * jax.random.uniform(streams_of[7], (HEAD_COUNT * HEAD_WIDTH,), jnp.float32) ** levels(streams_of[7], (HEAD_COUNT * HEAD_WIDTH,), ((0, 4),), -0.2, 0.2), -3.0, 0.5)
    correction_offset = jnp.clip(jax.random.uniform(streams_of[8], (HEAD_COUNT * HEAD_WIDTH,), jnp.float32, -2.0, 2.0) * levels(streams_of[8], (HEAD_COUNT * HEAD_WIDTH,), ((0, 4),), -0.4, 0.0), -2.0, 2.0)
    correction_key_factor = jnp.clip(jax.random.uniform(streams_of[9], (HEAD_COUNT * HEAD_WIDTH,), jnp.float32, -1.0, 1.0) * levels(streams_of[9], (HEAD_COUNT * HEAD_WIDTH,), ((0, 4),), -0.4, 0.0), -1.0, 1.0)
    own_term_weight = bell_draw(streams_of[10], (HEAD_COUNT * HEAD_WIDTH,), 0.15, 0.9, ((0, 4),), jnp.float32)
    head_norm_gain = jnp.clip(1.0 + 0.18 * jax.random.normal(streams_of[11], (HEAD_COUNT * HEAD_WIDTH,), jnp.float32), 0.1, 1.9)
    output_matrix = bell_draw(streams_of[12], (HEAD_COUNT * HEAD_WIDTH, D), (HEAD_COUNT * HEAD_WIDTH) ** -0.5, 0.1875, ((0, 4),))
    second_norm_gain = jnp.clip(1.0 + 0.18 * jax.random.normal(streams_of[13], (D,), jnp.float32), 0.1, 1.9)
    routing_keys = jax.random.split(jax.random.fold_in(streams_of[14], 1), B_TOT // B_DEV)
    routing_turns = jax.random.permutation(jax.random.fold_in(streams_of[14], 3), B_TOT // B_DEV)
    routing = jax.vmap(lambda own, number: shared_out(jax.random.fold_in(streams_of[14], 2), own, number, B_DEV, EXPERTS, TOP_K, CAP, 2))(routing_keys, routing_turns).reshape((B_TOT, TOP_K))
    routing_weight = jnp.clip(0.1 + 0.9 * jax.random.uniform(streams_of[15], (B_TOT, TOP_K), jnp.float32) ** levels(streams_of[15], (B_TOT, TOP_K), ((0, 8),), -0.2, 0.2), 0.1, 1.0)
    expert_gate_weight = bell_draw(streams_of[16], (EXPERTS, D, FF_E), D ** -0.5, 0.125, ((0, 8), (2, 4)))
    expert_up_weight = bell_draw(streams_of[17], (EXPERTS, D, FF_E), D ** -0.5, 0.125, ((0, 8), (2, 4)))
    expert_down_weight = gaussian_with(streams_of[18], (EXPERTS, FF_E, D), FF_E ** -0.5, 0.125, ((0, 8), (1, 4)), (1, 2, 4, 2.0))
    dense_gate_weight = bell_draw(streams_of[19], (D, FF_D), D ** -0.5, 0.125, ((1, 8),))
    dense_up_weight = bell_draw(streams_of[20], (D, FF_D), D ** -0.5, 0.125, ((1, 8),))
    dense_down_weight = bell_draw(streams_of[21], (FF_D, D), FF_D ** -0.5, 0.109375, ((0, 8),))
    dense_gate_offset = jnp.clip(jax.random.uniform(streams_of[22], (D,), jnp.float32, -3.0, 3.0), -3.0, 3.0)
    return {"tokens": tokens, "recurrent_head_state": recurrent_head_state, "first_norm_gain": first_norm_gain, "receptance_matrix": receptance_matrix, "key_matrix": key_matrix, "value_matrix": value_matrix, "decay_matrix": decay_matrix, "decay_offset": decay_offset, "correction_offset": correction_offset, "correction_key_factor": correction_key_factor, "own_term_weight": own_term_weight, "head_norm_gain": head_norm_gain, "output_matrix": output_matrix, "second_norm_gain": second_norm_gain, "routing": routing, "routing_weight": routing_weight, "expert_gate_weight": expert_gate_weight, "expert_up_weight": expert_up_weight, "expert_down_weight": expert_down_weight, "dense_gate_weight": dense_gate_weight, "dense_up_weight": dense_up_weight, "dense_down_weight": dense_down_weight, "dense_gate_offset": dense_gate_offset}


PRECISE = lax.Precision.HIGHEST

def rms_scale(rows, gain):
    floats = rows.astype(jnp.float32)
    return floats * lax.rsqrt(lax.optimization_barrier(jnp.mean(floats * floats, axis=-1, keepdims=True)) + 1e-06) * gain

def route_table(block_routes, experts, capacity):
    flat_routes = block_routes.reshape(-1)
    chosen = (flat_routes[:, None] == jnp.arange(experts, dtype=jnp.int32)[None, :]).astype(jnp.int32)
    before = jnp.cumsum(chosen, axis=0, dtype=jnp.int32) - chosen
    slot_index = lax.optimization_barrier(jnp.sum(before * chosen, axis=1))
    slot_match = (slot_index[:, None] == jnp.arange(capacity, dtype=jnp.int32)[None, :]).astype(jnp.float32)
    dispatch_table = chosen.astype(jnp.float32)[:, :, None] * slot_match[:, None, :]
    return dispatch_table.reshape(block_routes.shape[0], block_routes.shape[1], experts, capacity)

def state_update(receptance_rows, key_matrix_rows, value_matrix_rows, decay_logits, recurrent_head_state, decay_offset, correction_offset, correction_key_factor, own_term_weight, head_norm_gain, head_width):
    seq_count = key_matrix_rows.shape[0]
    decay_factor = jnp.exp(-jnp.exp(decay_offset + decay_logits))
    in_rate = jax.nn.sigmoid(correction_offset + correction_key_factor * key_matrix_rows)
    key_in = key_matrix_rows * in_rate

    def split_heads(block):
        return block.reshape(seq_count, -1, head_width)
    keys_head = split_heads(key_matrix_rows)
    unit_keys = keys_head * lax.rsqrt(lax.optimization_barrier(jnp.mean(keys_head * keys_head, axis=-1, keepdims=True)) + 1e-06) * head_width ** (-0.5)
    rate_head = split_heads(in_rate)
    head_keys = split_heads(key_in)
    decay_head = split_heads(decay_factor)
    head_values = split_heads(value_matrix_rows)
    head_receptance = split_heads(receptance_rows)
    matrix = recurrent_head_state.reshape(seq_count, -1, head_width, head_width)
    removed = jnp.einsum('bhvk,bhk->bhv', matrix, unit_keys, precision=PRECISE)
    updated = matrix * decay_head[:, :, None, :] - removed[..., None] * (unit_keys * rate_head)[:, :, None, :] + head_values[..., None] * head_keys[:, :, None, :]
    readout = jnp.einsum('bhvk,bhk->bhv', updated, head_receptance, precision=PRECISE)
    center = lax.optimization_barrier(jnp.mean(readout, axis=-1, keepdims=True))
    spread = lax.optimization_barrier(jnp.mean(jnp.square(readout - center), axis=-1, keepdims=True))
    normalized_rows = (readout - center) * lax.rsqrt(spread + 0.00064) * head_norm_gain.reshape(-1, head_width)
    own_term_total = lax.optimization_barrier(jnp.sum(head_receptance * head_keys * own_term_weight.reshape(-1, head_width), axis=-1, keepdims=True))
    normalized_rows = normalized_rows + own_term_total * head_values
    return (normalized_rows.reshape(seq_count, -1).astype(jnp.bfloat16), updated.reshape(seq_count, -1, head_width * head_width))

def reference(tokens, recurrent_head_state, first_norm_gain, receptance_matrix, key_matrix, value_matrix, decay_matrix, decay_offset, correction_offset, correction_key_factor, own_term_weight, head_norm_gain, output_matrix, second_norm_gain, routing, routing_weight, expert_gate_weight, expert_up_weight, expert_down_weight, dense_gate_weight, dense_up_weight, dense_down_weight, dense_gate_offset):
    normalized_rows = rms_scale(tokens, first_norm_gain).astype(jnp.bfloat16)
    receptance_rows = jnp.dot(normalized_rows, receptance_matrix, preferred_element_type=jnp.float32)
    key_matrix_rows = jnp.dot(normalized_rows, key_matrix, preferred_element_type=jnp.float32)
    value_matrix_rows = jnp.dot(normalized_rows, value_matrix, preferred_element_type=jnp.float32)
    decay_logits = jnp.dot(normalized_rows, decay_matrix, preferred_element_type=jnp.float32)
    head_outputs, next_state = state_update(receptance_rows, key_matrix_rows, value_matrix_rows, decay_logits, recurrent_head_state, decay_offset, correction_offset, correction_key_factor, own_term_weight, head_norm_gain, HEAD_WIDTH)
    hidden_sum = tokens.astype(jnp.float32) + jnp.dot(head_outputs, output_matrix, preferred_element_type=jnp.float32)
    ffn_in = rms_scale(hidden_sum, second_norm_gain).astype(jnp.bfloat16)
    tables = jax.vmap(partial(route_table, experts=EXPERTS, capacity=CAP))(routing.reshape(N_EP, B_DEV, TOP_K))
    grouped = ffn_in.reshape(N_EP, B_DEV, D).astype(jnp.float32)
    buffers = jnp.einsum('sbkec,sbd->escd', tables, grouped, precision=PRECISE).astype(jnp.bfloat16)

    def one_expert(packed):
        rows, gate_part, up_part, down_part = packed
        flat_rows = rows.reshape(-1, D)
        gate_pre = jnp.dot(flat_rows, gate_part, preferred_element_type=jnp.float32)
        up_pre = jnp.dot(flat_rows, up_part, preferred_element_type=jnp.float32)
        hidden = (jax.nn.silu(gate_pre) * up_pre).astype(jnp.bfloat16)
        result = jnp.dot(hidden, down_part, preferred_element_type=jnp.float32).astype(jnp.bfloat16)
        return result.reshape(rows.shape)
    expert_outs = lax.map(one_expert, (buffers, expert_gate_weight, expert_up_weight, expert_down_weight))
    weighted = jnp.einsum('sbkec,sbk->secb', tables, routing_weight.reshape(N_EP, B_DEV, TOP_K), precision=PRECISE)
    moe = jnp.einsum('secb,escd->sbd', weighted, expert_outs.astype(jnp.float32), precision=PRECISE).reshape(B_TOT, D)
    dense_hidden = (jax.nn.silu(jnp.dot(ffn_in, dense_gate_weight, preferred_element_type=jnp.float32)) * jnp.dot(ffn_in, dense_up_weight, preferred_element_type=jnp.float32)).astype(jnp.bfloat16)
    block_units = FF_D // N_EP

    def add_block(total, index):
        start = index * block_units
        piece = lax.dynamic_slice_in_dim(dense_hidden, start, block_units, 1)
        rows = lax.dynamic_slice_in_dim(dense_down_weight, start, block_units, 0)
        part = jnp.dot(piece, rows, preferred_element_type=jnp.float32).astype(jnp.bfloat16)
        part = lax.optimization_barrier(part)
        return (total + part.astype(jnp.float32), None)
    dense_sum, _ = lax.scan(add_block, jnp.zeros((B_TOT, D), jnp.float32), jnp.arange(N_EP, dtype=jnp.int32))
    layer_out = (hidden_sum + moe + jax.nn.sigmoid(dense_gate_offset) * dense_sum).astype(jnp.bfloat16)
    return (layer_out, next_state)
```

```python
import functools

import jax
import jax.numpy as jnp
from jax import lax
from jax.experimental import pallas as pl
from jax.experimental.pallas import tpu as pltpu
from jax.sharding import PartitionSpec as P

HEAD_WIDTH = 64
VMEM_BYTES = 67043328


PRECISE = lax.Precision.HIGHEST


def rms_scale(rows, gain):
    floats = rows.astype(jnp.float32)
    return floats * lax.rsqrt(jnp.mean(floats * floats, axis=-1, keepdims=True) + 1e-06) * gain


def route_table(block_routes, experts, capacity):
    flat_routes = block_routes.reshape(-1)
    chosen = (flat_routes[:, None] == jnp.arange(experts, dtype=jnp.int32)[None, :]).astype(
        jnp.int32
    )
    before = jnp.cumsum(chosen, axis=0, dtype=jnp.int32) - chosen
    slot_index = jnp.sum(before * chosen, axis=1)
    slot_match = (slot_index[:, None] == jnp.arange(capacity, dtype=jnp.int32)[None, :]).astype(
        jnp.float32
    )
    dispatch_table = chosen.astype(jnp.float32)[:, :, None] * slot_match[:, None, :]
    return dispatch_table.reshape(block_routes.shape[0], block_routes.shape[1], experts, capacity)


def state_update(
    receptance_rows,
    key_matrix_rows,
    value_matrix_rows,
    decay_logits,
    recurrent_head_state,
    decay_offset,
    correction_offset,
    correction_key_factor,
    own_term_weight,
    head_norm_gain,
    head_width,
):
    seq_count = key_matrix_rows.shape[0]
    decay_factor = jnp.exp(-jnp.exp(decay_offset + decay_logits))
    in_rate = jax.nn.sigmoid(correction_offset + correction_key_factor * key_matrix_rows)
    key_in = key_matrix_rows * in_rate

    def split_heads(block):
        return block.reshape(seq_count, -1, head_width)

    keys_head = split_heads(key_matrix_rows)
    unit_keys = (
        keys_head
        * lax.rsqrt(jnp.mean(keys_head * keys_head, axis=-1, keepdims=True) + 1e-06)
        * head_width ** (-0.5)
    )
    rate_head = split_heads(in_rate)
    head_keys = split_heads(key_in)
    decay_head = split_heads(decay_factor)
    head_values = split_heads(value_matrix_rows)
    head_receptance = split_heads(receptance_rows)
    matrix = recurrent_head_state.reshape(seq_count, -1, head_width, head_width)
    removed = jnp.einsum("bhvk,bhk->bhv", matrix, unit_keys, precision=PRECISE)
    updated = (
        matrix * decay_head[:, :, None, :]
        - removed[..., None] * (unit_keys * rate_head)[:, :, None, :]
        + head_values[..., None] * head_keys[:, :, None, :]
    )
    readout = jnp.einsum("bhvk,bhk->bhv", updated, head_receptance, precision=PRECISE)
    center = jnp.mean(readout, axis=-1, keepdims=True)
    spread = jnp.mean(jnp.square(readout - center), axis=-1, keepdims=True)
    normalized_rows = (
        (readout - center) * lax.rsqrt(spread + 0.00064) * head_norm_gain.reshape(-1, head_width)
    )
    own_term_total = jnp.sum(
        head_receptance * head_keys * own_term_weight.reshape(-1, head_width),
        axis=-1,
        keepdims=True,
    )
    normalized_rows = normalized_rows + own_term_total * head_values
    return (
        normalized_rows.reshape(seq_count, -1).astype(jnp.bfloat16),
        updated.reshape(seq_count, -1, head_width * head_width),
    )


def local(
    tokens,
    recurrent_head_state,
    first_norm_gain,
    receptance_matrix,
    key_matrix,
    value_matrix,
    decay_matrix,
    decay_offset,
    correction_offset,
    correction_key_factor,
    own_term_weight,
    head_norm_gain,
    output_matrix,
    second_norm_gain,
    routing,
    routing_weight,
    expert_gate_weight,
    expert_up_weight,
    expert_down_weight,
    dense_gate_weight,
    dense_up_weight,
    dense_down_weight,
    dense_gate_offset,
):
    seq_count = tokens.shape[0]
    width = tokens.shape[1]
    group_index = lax.axis_index("ep")
    lane_index = lax.axis_index("tp")
    group_count = lax.axis_size("ep")
    lane_count = lax.axis_size("tp")
    normalized_rows = rms_scale(tokens, first_norm_gain).astype(jnp.bfloat16)
    receptance_rows = jnp.dot(
        normalized_rows, receptance_matrix, preferred_element_type=jnp.float32
    )
    key_matrix_rows = jnp.dot(normalized_rows, key_matrix, preferred_element_type=jnp.float32)
    value_matrix_rows = jnp.dot(normalized_rows, value_matrix, preferred_element_type=jnp.float32)
    decay_logits = jnp.dot(normalized_rows, decay_matrix, preferred_element_type=jnp.float32)
    head_outputs, next_state = state_update(
        receptance_rows,
        key_matrix_rows,
        value_matrix_rows,
        decay_logits,
        recurrent_head_state,
        decay_offset,
        correction_offset,
        correction_key_factor,
        own_term_weight,
        head_norm_gain,
        HEAD_WIDTH,
    )
    partial_out = jnp.dot(head_outputs, output_matrix, preferred_element_type=jnp.float32)
    hidden_sum = tokens.astype(jnp.float32) + lax.psum(
        partial_out.astype(jnp.bfloat16), "tp"
    ).astype(jnp.float32)
    ffn_in = rms_scale(hidden_sum, second_norm_gain).astype(jnp.bfloat16)
    local_experts = expert_gate_weight.shape[0]
    top_count = routing.shape[1]
    expert_count = local_experts * group_count
    capacity = 2 * seq_count * top_count // expert_count
    per_lane = seq_count // lane_count
    own_routes = lax.dynamic_slice_in_dim(routing, group_index * seq_count, seq_count, 0)
    own_table = route_table(own_routes, expert_count, capacity)
    send_rows = jnp.einsum(
        "bkec,bd->ecd", own_table.astype(jnp.bfloat16), ffn_in, preferred_element_type=jnp.float32
    ).astype(jnp.bfloat16)
    lane_rows = lax.dynamic_slice_in_dim(ffn_in, lane_index * per_lane, per_lane, 0)
    dense_send = jnp.broadcast_to(lane_rows[None], (group_count, per_lane, width))
    expert_in, dense_in = (
        lax.all_to_all(send_rows, "ep", split_axis=0, concat_axis=0, tiled=True),
        lax.all_to_all(dense_send, "ep", split_axis=0, concat_axis=0, tiled=True),
    )
    rows_in = expert_in.reshape(group_count, local_experts, capacity, width).transpose(1, 0, 2, 3)
    rows_in = rows_in.reshape(local_experts, group_count * capacity, width)
    gate_pre = jnp.einsum(
        "lrd,ldf->lrf", rows_in, expert_gate_weight, preferred_element_type=jnp.float32
    )
    up_pre = jnp.einsum(
        "lrd,ldf->lrf", rows_in, expert_up_weight, preferred_element_type=jnp.float32
    )
    expert_hidden = (jax.nn.silu(gate_pre) * up_pre).astype(jnp.bfloat16)
    expert_part = jnp.einsum(
        "lrf,lfd->lrd", expert_hidden, expert_down_weight, preferred_element_type=jnp.float32
    )
    expert_out = lax.psum_scatter(
        expert_part.astype(jnp.bfloat16), "tp", scatter_dimension=2, tiled=True
    )
    back_send = expert_out.reshape(local_experts, group_count, capacity, -1).transpose(1, 0, 2, 3)
    back_send = back_send.reshape(group_count * local_experts, capacity, -1)
    dense_rows = dense_in.reshape(group_count * per_lane, width)
    dense_hidden = (
        jax.nn.silu(jnp.dot(dense_rows, dense_gate_weight, preferred_element_type=jnp.float32))
        * jnp.dot(dense_rows, dense_up_weight, preferred_element_type=jnp.float32)
    ).astype(jnp.bfloat16)
    dense_part = jnp.dot(
        dense_hidden, dense_down_weight, preferred_element_type=jnp.float32
    ).astype(jnp.bfloat16)
    dense_part = dense_part.reshape(group_count, per_lane, width)
    back_experts, back_dense = (
        lax.all_to_all(back_send, "ep", split_axis=0, concat_axis=0, tiled=True),
        lax.all_to_all(dense_part, "ep", split_axis=0, concat_axis=0, tiled=True),
    )
    dense_sum = jnp.sum(back_dense.astype(jnp.float32), axis=0)
    weighted = jnp.einsum("bkec,bk->ecb", own_table, routing_weight, precision=PRECISE)
    moe_slice = jnp.einsum(
        "ecb,ecd->bd", weighted, back_experts.astype(jnp.float32), precision=PRECISE
    )
    moe_rows = lax.all_to_all(moe_slice, "tp", split_axis=0, concat_axis=1, tiled=True)
    residual_rows = lax.dynamic_slice_in_dim(hidden_sum, lane_index * per_lane, per_lane, 0)
    layer_out = (residual_rows + moe_rows + jax.nn.sigmoid(dense_gate_offset) * dense_sum).astype(
        jnp.bfloat16
    )
    return (layer_out, next_state)


def fused_kernel(count, groups, lanes, *refs):
    sources, refs = refs[:count], refs[count:]
    state_ref, gain_hbm, goff_hbm, eg_hbm, eu_hbm, ed_hbm, dg_hbm, du_hbm, dd_hbm = refs[:9]
    nbuf, out_ref = refs[9:11]
    held, refs = refs[11 : 11 + count], refs[11 + count :]
    (tokens_ref, gain_ref, doff_ref, coff_ref, cfac_ref, own_ref, hgain_ref, routes_ref,
     rweight_ref, wk_ref, wd_ref, wr_ref, wv_ref, wo_ref) = held
    (sbuf, pbuf, gather_ones, spread_ones, spread_in,
     eg, eu, ed, dg, du, dd, gain, goff, part_ref, hid_rows, p_in, xs, flat, hid, dens,
     ys, y_in, z_in, v_out, v_in,
     arg_sem, in_sem,
     w_sem, s1, r1, sz, rz, st, rt, sc, rc, sa, ra, sb, rb, sv, rv) = refs
    f32, bf16 = jnp.float32, jnp.bfloat16
    zs = groups // 2
    me_g, me_l = lax.axis_index("ep"), lax.axis_index("tp")
    core, me_z = lax.rem(me_g, 2), me_g // 2
    partner = (me_g + 1 - 2 * core, me_l)

    def lane_peer(d):
        return (me_g, lax.rem(me_l + d + lanes, lanes))

    def z_peer(d):
        return (lax.rem(me_z + d + zs, zs) * 2 + core, me_l)

    def send(src, dst, ssem, rsem, peer):
        copy = pltpu.make_async_remote_copy(
            src_ref=src, dst_ref=dst, send_sem=ssem, recv_sem=rsem, device_id=peer,
            device_id_type=pl.DeviceIdType.MESH,
        )
        copy.start()
        return copy

    seqs, width = tokens_ref.shape
    heads = state_ref.shape[1]
    rows = seqs // lanes
    args = [
        pltpu.make_async_copy(src, dst, arg_sem.at[i])
        for i, (src, dst) in enumerate(zip(sources, held))
    ]
    loads = [
        pltpu.make_async_copy(state_ref.at[:, h, :], sbuf.at[h], in_sem.at[h]) for h in range(heads)
    ]
    for arg in args[:-2]:
        arg.start()
    for load in loads:
        load.start()
    for arg in args[-2:]:
        arg.start()
    barrier = pltpu.get_barrier_semaphore()
    peers = [lane_peer(d) for d in range(1, lanes)] + [z_peer(d) for d in range(1, zs)] + [partner]
    for peer in peers:
        pl.semaphore_signal(barrier, inc=1, device_id=peer, device_id_type=pl.DeviceIdType.MESH)

    pair = 2 * HEAD_WIDTH
    flat_width = state_ref.shape[2]
    tile = 256

    @pl.loop(0, flat_width // tile)
    def _(n):
        at = pl.multiple_of(n * tile, tile)
        r = (lax.broadcasted_iota(jnp.int32, (tile, pair), 0) + at) // HEAD_WIDTH
        c = lax.broadcasted_iota(jnp.int32, (tile, pair), 1) % HEAD_WIDTH
        gather_ones[pl.ds(at, tile), :] = (r == c).astype(f32).astype(bf16)
        r = lax.broadcasted_iota(jnp.int32, (pair, tile), 0) % HEAD_WIDTH
        c = (lax.broadcasted_iota(jnp.int32, (pair, tile), 1) + at) // HEAD_WIDTH
        spread_ones[:, pl.ds(at, tile)] = (r == c).astype(f32).astype(bf16)

    half_r = lax.broadcasted_iota(jnp.int32, (pair, pair), 0) // HEAD_WIDTH
    half_c = lax.broadcasted_iota(jnp.int32, (pair, pair), 1) // HEAD_WIDTH
    ones_block = (half_r == half_c).astype(f32).astype(bf16)

    def group_sums(*blocks):
        parts = []
        for block in blocks:
            for i in range(0, block.shape[1], pair):
                piece = block[:, i : i + pair]
                high = piece.astype(bf16)
                parts += [high, (piece - high.astype(f32)).astype(bf16)]
        made = jnp.dot(jnp.concatenate(parts, axis=0), ones_block, preferred_element_type=f32)
        sums, at = [], 0
        for block in blocks:
            cols = []
            for i in range(0, block.shape[1], pair):
                cols.append(made[at : at + seqs] + made[at + seqs : at + 2 * seqs])
                at += 2 * seqs
            sums.append(jnp.concatenate(cols, axis=1))
        return sums

    lane = lax.broadcasted_iota(jnp.int32, (seqs, pair), 1)
    low = lane < HEAD_WIDTH

    def doubled(full, h):
        chunk = full[:, (h // 2) * pair : (h // 2 + 1) * pair]
        turned = pltpu.roll(chunk, HEAD_WIDTH, 1)
        return jnp.where(low, chunk, turned) if h % 2 == 0 else jnp.where(low, turned, chunk)

    for arg in args[:9]:
        arg.wait()
    toks = tokens_ref[...].astype(f32)
    normed = (
        toks * lax.rsqrt(jnp.mean(toks * toks, axis=-1, keepdims=True) + 1e-06) * gain_ref[...]
    ).astype(bf16)
    start = me_g * seqs + me_l * rows

    def picked_column(ref, k, first):
        spot = lax.broadcasted_iota(jnp.int32, (rows, ref.shape[1]), 1)
        wanted = spot == first + lax.broadcasted_iota(jnp.int32, spot.shape, 0)
        entries = ref[k : k + 1, :].astype(f32)
        return jnp.sum(jnp.where(wanted, entries, 0.0), axis=-1, keepdims=True)

    column = lax.broadcasted_iota(jnp.int32, (rows, 128), 1) % 64
    column = column.astype(f32)
    table = jnp.zeros((rows, 128), f32)
    for k in range(routes_ref.shape[0]):
        expert = picked_column(routes_ref, k, start)
        table = table + jnp.where(
            column == expert, picked_column(rweight_ref, k, me_l * rows), 0.0
        )
    high = table.astype(bf16).astype(f32)
    first_half = lax.broadcasted_iota(jnp.int32, table.shape, 1) < 64
    xs[0, 0, 0, :, width:] = jnp.where(first_half, high, table - high).astype(bf16)

    args[9].wait()
    keys = jnp.dot(normed, wk_ref[...], preferred_element_type=f32)
    (key_squares,) = group_sums(keys * keys)
    rate = jax.nn.sigmoid(coff_ref[...] + cfac_ref[...] * keys)
    unit = keys * lax.rsqrt(key_squares * (1.0 / HEAD_WIDTH) + 1e-06) * HEAD_WIDTH ** (-0.5)
    key_in = keys * rate
    back = unit * rate
    args[10].wait()
    logits = jnp.dot(normed, wd_ref[...], preferred_element_type=f32)
    decay = jnp.exp(-jnp.exp(doff_ref[...] + logits))
    args[11].wait()
    recept = jnp.dot(normed, wr_ref[...], preferred_element_type=f32)
    faded = decay * recept
    back_sum, in_sum, own_sum = group_sums(
        back * recept, key_in * recept, recept * key_in * own_ref[...]
    )
    for h in range(heads):
        u2, f2 = doubled(unit, h), doubled(faded, h)
        loads[h].wait()
        for j in range(0, flat_width, pair):
            old = sbuf[h, :, j : j + pair]
            pbuf[2 * h * seqs : (2 * h + 1) * seqs, j : j + pair] = (old * u2).astype(bf16)
            pbuf[(2 * h + 1) * seqs : (2 * h + 2) * seqs, j : j + pair] = (old * f2).astype(bf16)
    sums = jnp.dot(pbuf[...], gather_ones[...], preferred_element_type=f32)
    args[12].wait()
    values = jnp.dot(normed, wv_ref[...], preferred_element_type=f32)

    def merged(first):
        picks = [sums[(2 * h + first) * seqs : (2 * h + first + 1) * seqs] for h in range(heads)]
        return jnp.concatenate(
            [jnp.where(low, picks[h], picks[h + 1]) for h in range(0, heads, 2)], axis=1
        )

    read = merged(1) - merged(0) * back_sum + values * in_sum
    (read_sum,) = group_sums(read)
    center = read - read_sum * (1.0 / HEAD_WIDTH)
    (square_sum,) = group_sums(center * center)
    heads_out = (
        center * lax.rsqrt(square_sum * (1.0 / HEAD_WIDTH) + 0.00064) * hgain_ref[...]
        + own_sum * values
    ).astype(bf16)
    args[13].wait()
    part = jnp.dot(heads_out, wo_ref[...], preferred_element_type=f32)
    base = jnp.zeros((rows, width), f32)
    for i in range(lanes):
        mine = part[i * rows : (i + 1) * rows]
        part_ref[i] = mine.astype(bf16)
        base = jnp.where(me_l == i, mine + toks[i * rows : (i + 1) * rows], base)
    hid_rows[...] = base
    pl.semaphore_wait(barrier, len(peers))
    sent = []
    firsts = []
    for d in range(1, lanes):
        target = lax.rem(me_l + lanes - d, lanes)
        firsts.append(
            send(part_ref.at[target], p_in.at[d - 1], s1.at[d - 1], r1.at[d - 1], (me_g, target))
        )
    pulls = [
        pltpu.make_async_copy(src, dst, w_sem.at[i])
        for i, (src, dst) in enumerate(
            [(gain_hbm, gain), (goff_hbm, goff), (dg_hbm, dg), (du_hbm, du), (dd_hbm, dd),
             (eg_hbm.at[0], eg), (eu_hbm.at[0], eu), (ed_hbm.at[0], ed)]
        )
    ]
    for pull in pulls:
        pull.start()

    def halves(block):
        high = block.astype(bf16).astype(f32)
        return jnp.where(low, high, block - high).astype(bf16)

    for h in range(heads):
        spread_in[2 * h * seqs : (2 * h + 1) * seqs] = halves(
            sums[2 * h * seqs : (2 * h + 1) * seqs]
        )
        spread_in[(2 * h + 1) * seqs : (2 * h + 2) * seqs] = halves(doubled(values, h))
    fades = [doubled(decay, h) for h in range(heads)]
    backs = [doubled(back, h) for h in range(heads)]
    ins = [doubled(key_in, h) for h in range(heads)]
    for n in range(0, flat_width, tile):
        wide_rows = jnp.dot(
            spread_in[...], spread_ones[:, n : n + tile], preferred_element_type=f32
        )
        for h in range(heads):
            gone = wide_rows[2 * h * seqs : (2 * h + 1) * seqs]
            came = wide_rows[(2 * h + 1) * seqs : (2 * h + 2) * seqs]
            for i in range(0, tile, pair):
                nbuf[h, :, n + i : n + i + pair] = (
                    sbuf[h, :, n + i : n + i + pair] * fades[h]
                    - gone[:, i : i + pair] * backs[h]
                    + came[:, i : i + pair] * ins[h]
                )
    hidden = hid_rows[...]
    for d, copy in enumerate(firsts):
        copy.wait_recv()
        hidden = hidden + p_in[d].astype(f32)
    sent += firsts
    hid_rows[...] = hidden
    for pull in pulls[:2]:
        pull.wait()
    normed = hidden * lax.rsqrt(jnp.mean(hidden * hidden, axis=-1, keepdims=True) + 1e-06)
    xs[0, 0, 0, :, :width] = (normed * gain[...]).astype(bf16)
    hold_z, hold_t, hold_c = {}, {}, {}
    for d in range(1, zs):
        hold_z[d] = send(xs.at[0, 0, 0], xs.at[0, 0, d], sz.at[d - 1], rz.at[d - 1], z_peer(d))

    def to_partner(d, q):
        i = d * zs + q
        hold_c[d, q] = send(xs.at[0, d, q], xs.at[1, d, q], sc.at[i], rc.at[i], partner)

    def to_lanes(q):
        to_partner(0, q)
        for d in range(1, lanes):
            i = (d - 1) * zs + q
            hold_t[d, q] = send(xs.at[0, 0, q], xs.at[0, d, q], st.at[i], rt.at[i], lane_peer(d))

    to_lanes(0)
    for q in range(1, zs):
        hold_z[q].wait_recv()
        to_lanes(q)
    block = 2 * zs * rows

    def gathered(d):
        return xs[:, d].astype(f32).reshape(block, width + 128)

    for q in range(zs):
        hold_c[0, q].wait_recv()
    mine = gathered(0)
    flat[0:block] = mine.astype(bf16)
    own_rows = mine[:, :width].astype(bf16)
    for pull in pulls[2:5]:
        pull.wait()
    across = (((1,), (1,)), ((), ()))
    gate = lax.dot_general(own_rows, dg[...], across, preferred_element_type=f32)
    up = lax.dot_general(own_rows, du[...], across, preferred_element_type=f32)
    mixed = (jax.nn.silu(gate) * up).astype(bf16)
    dens[...] = jnp.dot(mixed, dd[...], preferred_element_type=f32) * jax.nn.sigmoid(goff[...])
    for q in range(zs):
        for d in range(1, lanes):
            hold_t[d, q].wait_recv()
            to_partner(d, q)
    for d in range(1, lanes):
        for q in range(zs):
            hold_c[d, q].wait_recv()
        flat[d * block : (d + 1) * block] = gathered(d).astype(bf16)
    for pull in pulls[5:]:
        pull.wait()

    @pl.loop(0, eg.shape[1] // tile, unroll=True)
    def _(n):
        cols = pl.ds(pl.multiple_of(n * tile, tile), tile)
        left = flat[:, :width]
        gated = jnp.dot(left, eg[:, cols], preferred_element_type=f32)
        raised = jnp.dot(left, eu[:, cols], preferred_element_type=f32)
        hid[:, cols] = (jax.nn.silu(gated) * raised).astype(bf16)

    tail = flat[:, width:].astype(f32)
    picked = lax.broadcasted_iota(jnp.int32, tail.shape, 1) % 64 == me_g
    scale = jnp.sum(jnp.where(picked, tail, 0.0), axis=-1, keepdims=True)
    pieces, wide = ys.shape[0], ys.shape[-1]
    to_core, to_lane, to_z = [], [], []

    def pass_on(n):
        to_core[n].wait_recv()
        own = []
        for d in range(1, lanes):
            ys[n, 0, d] = (ys[n, 0, d].astype(f32) + y_in[n, d].astype(f32)).astype(bf16)
            i = n * (lanes - 1) + d - 1
            own.append(
                send(ys.at[n, 0, d], z_in.at[n, d - 1], sb.at[i], rb.at[i], lane_peer(-d))
            )
        to_lane.append(own)

    for n in range(pieces):
        cols = slice(n * wide, (n + 1) * wide)
        made = jnp.dot(hid[...], ed[:, cols], preferred_element_type=f32) * scale
        for d in range(lanes):
            piece = made[d * block : (d + 1) * block]
            if d == 0:
                piece = piece + dens[:, cols]
            ys[n, :, d] = piece.reshape(2, zs, rows, wide).astype(bf16)
        to_core.append(send(ys.at[n, 1], y_in.at[n], sa.at[n], ra.at[n], partner))
        if n > 0:
            pass_on(n - 1)
    pass_on(pieces - 1)
    for n in range(pieces):
        cols = slice(n * wide, (n + 1) * wide)
        total = ys[n, 0, 0].astype(f32) + y_in[n, 0].astype(f32)
        for d in range(1, lanes):
            to_lane[n][d - 1].wait_recv()
            total = total + z_in[n, d - 1].astype(f32)
        v_out[n] = total.astype(bf16)
        own = []
        for d in range(1, zs):
            i = n * (zs - 1) + d - 1
            own.append(
                send(v_out.at[n, d], v_in.at[n, d - 1], sv.at[i], rv.at[i], z_peer(-d))
            )
        to_z.append(own)
        hid_rows[:, cols] = hid_rows[:, cols] + total[0]
    for n in range(pieces):
        cols = slice(n * wide, (n + 1) * wide)
        result = hid_rows[:, cols]
        for d, copy in enumerate(to_z[n]):
            copy.wait_recv()
            result = result + v_in[n, d].astype(f32)
        out_ref[:, cols] = result.astype(bf16)
    sent += list(hold_z.values()) + list(hold_t.values()) + list(hold_c.values())
    sent += to_core
    for own in to_lane + to_z:
        sent += own
    for copy in sent:
        copy.wait_send()


def hand_over_kernel(rows_ref, state_ref, out_ref, next_ref, row_sem, state_sem):
    heads = state_ref.shape[0]
    copies = [pltpu.make_async_copy(rows_ref, out_ref, row_sem)] + [
        pltpu.make_async_copy(state_ref.at[h], next_ref.at[:, h, :], state_sem.at[h])
        for h in range(heads)
    ]
    for copy in copies:
        copy.start()
    for copy in copies:
        copy.wait()


def fused(
    tokens, recurrent_head_state, first_norm_gain, receptance_matrix, key_matrix, value_matrix,
    decay_matrix, decay_offset, correction_offset, correction_key_factor, own_term_weight,
    head_norm_gain, output_matrix, second_norm_gain, routing, routing_weight, expert_gate_weight,
    expert_up_weight, expert_down_weight, dense_gate_weight, dense_up_weight, dense_down_weight,
    dense_gate_offset,
):
    f32, bf16 = jnp.float32, jnp.bfloat16
    seqs, width = tokens.shape
    heads, flat_width = recurrent_head_state.shape[1:]
    groups, lanes = lax.axis_size("ep"), lax.axis_size("tp")
    rows, zs = seqs // lanes, groups // 2
    grant = VMEM_BYTES - rows * width * 2 - heads * seqs * flat_width * 4
    vmem = pl.BlockSpec(memory_space=pltpu.VMEM)
    anywhere = pl.BlockSpec(memory_space=pltpu.HBM)
    dma = pltpu.SemaphoreType.DMA

    def row(vector):
        return vector.reshape(1, -1)

    operands = (
        tokens, row(first_norm_gain), row(decay_offset), row(correction_offset),
        row(correction_key_factor), row(own_term_weight), row(head_norm_gain), routing.T,
        routing_weight.T, key_matrix, decay_matrix, receptance_matrix, value_matrix, output_matrix,
    )
    count = len(operands)
    hidden_units = expert_gate_weight.shape[2]
    pieces = 4
    wide = width // pieces
    total = groups * seqs
    pair = 2 * HEAD_WIDTH
    next_state, layer_rows = pl.pallas_call(
        functools.partial(fused_kernel, count, groups, lanes),
        out_shape=(
            jax.ShapeDtypeStruct((heads, seqs, flat_width), f32),
            jax.ShapeDtypeStruct((rows, width), bf16),
        ),
        in_specs=[anywhere] * (count + 9),
        out_specs=(vmem, vmem),
        scratch_shapes=[pltpu.VMEM(operand.shape, operand.dtype) for operand in operands]
        + [
            pltpu.VMEM((heads, seqs, flat_width), f32),
            pltpu.VMEM((2 * heads * seqs, flat_width), bf16),
            pltpu.VMEM((flat_width, pair), bf16),
            pltpu.VMEM((pair, flat_width), bf16),
            pltpu.VMEM((2 * heads * seqs, pair), bf16),
            pltpu.VMEM(expert_gate_weight.shape[1:], bf16),
            pltpu.VMEM(expert_up_weight.shape[1:], bf16),
            pltpu.VMEM(expert_down_weight.shape[1:], bf16),
            pltpu.VMEM(dense_gate_weight.shape[::-1], bf16),
            pltpu.VMEM(dense_up_weight.shape[::-1], bf16),
            pltpu.VMEM(dense_down_weight.shape, bf16),
            pltpu.VMEM((1, width), f32),
            pltpu.VMEM((1, width), f32),
            pltpu.VMEM((lanes, rows, width), bf16),
            pltpu.VMEM((rows, width), f32),
            pltpu.VMEM((lanes - 1, rows, width), bf16),
            pltpu.VMEM((2, lanes, zs, rows, width + 128), bf16),
            pltpu.VMEM((total, width + 128), bf16),
            pltpu.VMEM((total, hidden_units), bf16),
            pltpu.VMEM((2 * zs * rows, width), f32),
            pltpu.VMEM((pieces, 2, lanes, zs, rows, wide), bf16),
            pltpu.VMEM((pieces, lanes, zs, rows, wide), bf16),
            pltpu.VMEM((pieces, lanes - 1, zs, rows, wide), bf16),
            pltpu.VMEM((pieces, zs, rows, wide), bf16),
            pltpu.VMEM((pieces, zs - 1, rows, wide), bf16),
            dma((count,)),
            dma((heads,)),
            dma((8,)),
            dma((lanes - 1,)), dma((lanes - 1,)),
            dma((zs - 1,)), dma((zs - 1,)),
            dma(((lanes - 1) * zs,)), dma(((lanes - 1) * zs,)),
            dma((lanes * zs,)), dma((lanes * zs,)),
            dma((pieces,)), dma((pieces,)),
            dma((pieces * (lanes - 1),)), dma((pieces * (lanes - 1),)),
            dma((pieces * (zs - 1),)), dma((pieces * (zs - 1),)),
        ],
        compiler_params=pltpu.CompilerParams(
            collective_id=0, has_side_effects=True, vmem_limit_bytes=grant
        ),
        name="layer",
    )(
        *operands, recurrent_head_state, row(second_norm_gain), row(dense_gate_offset),
        expert_gate_weight, expert_up_weight, expert_down_weight, dense_gate_weight.T,
        dense_up_weight.T, dense_down_weight,
    )
    return pl.pallas_call(
        hand_over_kernel,
        out_shape=(
            jax.ShapeDtypeStruct((rows, width), bf16),
            jax.ShapeDtypeStruct(recurrent_head_state.shape, f32),
        ),
        in_specs=[vmem, vmem],
        out_specs=(anywhere, anywhere),
        scratch_shapes=[dma, dma((heads,))],
        name="hand_over",
    )(layer_rows, next_state)


def choose(tokens, recurrent_head_state, *rest):
    groups, lanes = lax.axis_size("ep"), lax.axis_size("tp")
    rows, heads = tokens.shape[0] // lanes, recurrent_head_state.shape[1]
    experts_here = rest[14].shape[0]
    fits = (
        rows % 8 == 0 and heads % 2 == 0 and groups % 2 == 0 and groups > 2 and lanes > 1
        and groups <= 64 and experts_here == 1
    )
    return (fused if fits else local)(tokens, recurrent_head_state, *rest)


def solution(mesh):
    return jax.shard_map(
        choose,
        mesh=mesh,
        in_specs=(
            P("ep", None),
            P("ep", "tp", None),
            P(),
            P(None, "tp"),
            P(None, "tp"),
            P(None, "tp"),
            P(None, "tp"),
            P("tp"),
            P("tp"),
            P("tp"),
            P("tp"),
            P("tp"),
            P("tp", None),
            P(),
            P(),
            P("ep", None),
            P("ep", None, "tp"),
            P("ep", None, "tp"),
            P("ep", "tp", None),
            P(None, "ep"),
            P(None, "ep"),
            P("ep", None),
            P(),
        ),
        out_specs=(P(("ep", "tp"), None), P("ep", "tp", None)),
        check_vma=False,
    )
```

```python
import functools

import jax
import jax.numpy as jnp
from jax import lax
from jax.experimental import pallas as pl
from jax.experimental.pallas import tpu as pltpu
from jax.sharding import PartitionSpec as P

HEAD_WIDTH = 64
VMEM_BYTES = 67043328


PRECISE = lax.Precision.HIGHEST


def rms_scale(rows, gain):
    floats = rows.astype(jnp.float32)
    return floats * lax.rsqrt(jnp.mean(floats * floats, axis=-1, keepdims=True) + 1e-06) * gain


def route_table(block_routes, experts, capacity):
    flat_routes = block_routes.reshape(-1)
    chosen = (flat_routes[:, None] == jnp.arange(experts, dtype=jnp.int32)[None, :]).astype(
        jnp.int32
    )
    before = jnp.cumsum(chosen, axis=0, dtype=jnp.int32) - chosen
    slot_index = jnp.sum(before * chosen, axis=1)
    slot_match = (slot_index[:, None] == jnp.arange(capacity, dtype=jnp.int32)[None, :]).astype(
        jnp.float32
    )
    dispatch_table = chosen.astype(jnp.float32)[:, :, None] * slot_match[:, None, :]
    return dispatch_table.reshape(block_routes.shape[0], block_routes.shape[1], experts, capacity)


def state_update(
    receptance_rows,
    key_matrix_rows,
    value_matrix_rows,
    decay_logits,
    recurrent_head_state,
    decay_offset,
    correction_offset,
    correction_key_factor,
    own_term_weight,
    head_norm_gain,
    head_width,
):
    seq_count = key_matrix_rows.shape[0]
    decay_factor = jnp.exp(-jnp.exp(decay_offset + decay_logits))
    in_rate = jax.nn.sigmoid(correction_offset + correction_key_factor * key_matrix_rows)
    key_in = key_matrix_rows * in_rate

    def split_heads(block):
        return block.reshape(seq_count, -1, head_width)

    keys_head = split_heads(key_matrix_rows)
    unit_keys = (
        keys_head
        * lax.rsqrt(jnp.mean(keys_head * keys_head, axis=-1, keepdims=True) + 1e-06)
        * head_width ** (-0.5)
    )
    rate_head = split_heads(in_rate)
    head_keys = split_heads(key_in)
    decay_head = split_heads(decay_factor)
    head_values = split_heads(value_matrix_rows)
    head_receptance = split_heads(receptance_rows)
    matrix = recurrent_head_state.reshape(seq_count, -1, head_width, head_width)
    removed = jnp.einsum("bhvk,bhk->bhv", matrix, unit_keys, precision=PRECISE)
    updated = (
        matrix * decay_head[:, :, None, :]
        - removed[..., None] * (unit_keys * rate_head)[:, :, None, :]
        + head_values[..., None] * head_keys[:, :, None, :]
    )
    readout = jnp.einsum("bhvk,bhk->bhv", updated, head_receptance, precision=PRECISE)
    center = jnp.mean(readout, axis=-1, keepdims=True)
    spread = jnp.mean(jnp.square(readout - center), axis=-1, keepdims=True)
    normalized_rows = (
        (readout - center) * lax.rsqrt(spread + 0.00064) * head_norm_gain.reshape(-1, head_width)
    )
    own_term_total = jnp.sum(
        head_receptance * head_keys * own_term_weight.reshape(-1, head_width),
        axis=-1,
        keepdims=True,
    )
    normalized_rows = normalized_rows + own_term_total * head_values
    return (
        normalized_rows.reshape(seq_count, -1).astype(jnp.bfloat16),
        updated.reshape(seq_count, -1, head_width * head_width),
    )


def local(
    tokens,
    recurrent_head_state,
    first_norm_gain,
    receptance_matrix,
    key_matrix,
    value_matrix,
    decay_matrix,
    decay_offset,
    correction_offset,
    correction_key_factor,
    own_term_weight,
    head_norm_gain,
    output_matrix,
    second_norm_gain,
    routing,
    routing_weight,
    expert_gate_weight,
    expert_up_weight,
    expert_down_weight,
    dense_gate_weight,
    dense_up_weight,
    dense_down_weight,
    dense_gate_offset,
):
    seq_count = tokens.shape[0]
    width = tokens.shape[1]
    group_index = lax.axis_index("ep")
    lane_index = lax.axis_index("tp")
    group_count = lax.axis_size("ep")
    lane_count = lax.axis_size("tp")
    normalized_rows = rms_scale(tokens, first_norm_gain).astype(jnp.bfloat16)
    receptance_rows = jnp.dot(
        normalized_rows, receptance_matrix, preferred_element_type=jnp.float32
    )
    key_matrix_rows = jnp.dot(normalized_rows, key_matrix, preferred_element_type=jnp.float32)
    value_matrix_rows = jnp.dot(normalized_rows, value_matrix, preferred_element_type=jnp.float32)
    decay_logits = jnp.dot(normalized_rows, decay_matrix, preferred_element_type=jnp.float32)
    head_outputs, next_state = state_update(
        receptance_rows,
        key_matrix_rows,
        value_matrix_rows,
        decay_logits,
        recurrent_head_state,
        decay_offset,
        correction_offset,
        correction_key_factor,
        own_term_weight,
        head_norm_gain,
        HEAD_WIDTH,
    )
    partial_out = jnp.dot(head_outputs, output_matrix, preferred_element_type=jnp.float32)
    hidden_sum = tokens.astype(jnp.float32) + lax.psum(
        partial_out.astype(jnp.bfloat16), "tp"
    ).astype(jnp.float32)
    ffn_in = rms_scale(hidden_sum, second_norm_gain).astype(jnp.bfloat16)
    local_experts = expert_gate_weight.shape[0]
    top_count = routing.shape[1]
    expert_count = local_experts * group_count
    capacity = 2 * seq_count * top_count // expert_count
    per_lane = seq_count // lane_count
    own_routes = lax.dynamic_slice_in_dim(routing, group_index * seq_count, seq_count, 0)
    own_table = route_table(own_routes, expert_count, capacity)
    send_rows = jnp.einsum(
        "bkec,bd->ecd", own_table.astype(jnp.bfloat16), ffn_in, preferred_element_type=jnp.float32
    ).astype(jnp.bfloat16)
    lane_rows = lax.dynamic_slice_in_dim(ffn_in, lane_index * per_lane, per_lane, 0)
    dense_send = jnp.broadcast_to(lane_rows[None], (group_count, per_lane, width))
    expert_in, dense_in = (
        lax.all_to_all(send_rows, "ep", split_axis=0, concat_axis=0, tiled=True),
        lax.all_to_all(dense_send, "ep", split_axis=0, concat_axis=0, tiled=True),
    )
    rows_in = expert_in.reshape(group_count, local_experts, capacity, width).transpose(1, 0, 2, 3)
    rows_in = rows_in.reshape(local_experts, group_count * capacity, width)
    gate_pre = jnp.einsum(
        "lrd,ldf->lrf", rows_in, expert_gate_weight, preferred_element_type=jnp.float32
    )
    up_pre = jnp.einsum(
        "lrd,ldf->lrf", rows_in, expert_up_weight, preferred_element_type=jnp.float32
    )
    expert_hidden = (jax.nn.silu(gate_pre) * up_pre).astype(jnp.bfloat16)
    expert_part = jnp.einsum(
        "lrf,lfd->lrd", expert_hidden, expert_down_weight, preferred_element_type=jnp.float32
    )
    expert_out = lax.psum_scatter(
        expert_part.astype(jnp.bfloat16), "tp", scatter_dimension=2, tiled=True
    )
    back_send = expert_out.reshape(local_experts, group_count, capacity, -1).transpose(1, 0, 2, 3)
    back_send = back_send.reshape(group_count * local_experts, capacity, -1)
    dense_rows = dense_in.reshape(group_count * per_lane, width)
    dense_hidden = (
        jax.nn.silu(jnp.dot(dense_rows, dense_gate_weight, preferred_element_type=jnp.float32))
        * jnp.dot(dense_rows, dense_up_weight, preferred_element_type=jnp.float32)
    ).astype(jnp.bfloat16)
    dense_part = jnp.dot(
        dense_hidden, dense_down_weight, preferred_element_type=jnp.float32
    ).astype(jnp.bfloat16)
    dense_part = dense_part.reshape(group_count, per_lane, width)
    back_experts, back_dense = (
        lax.all_to_all(back_send, "ep", split_axis=0, concat_axis=0, tiled=True),
        lax.all_to_all(dense_part, "ep", split_axis=0, concat_axis=0, tiled=True),
    )
    dense_sum = jnp.sum(back_dense.astype(jnp.float32), axis=0)
    weighted = jnp.einsum("bkec,bk->ecb", own_table, routing_weight, precision=PRECISE)
    moe_slice = jnp.einsum(
        "ecb,ecd->bd", weighted, back_experts.astype(jnp.float32), precision=PRECISE
    )
    moe_rows = lax.all_to_all(moe_slice, "tp", split_axis=0, concat_axis=1, tiled=True)
    residual_rows = lax.dynamic_slice_in_dim(hidden_sum, lane_index * per_lane, per_lane, 0)
    layer_out = (residual_rows + moe_rows + jax.nn.sigmoid(dense_gate_offset) * dense_sum).astype(
        jnp.bfloat16
    )
    return (layer_out, next_state)


def fused_kernel(count, groups, lanes, *refs):
    sources, refs = refs[:count], refs[count:]
    state_ref, gain_hbm, goff_hbm, eg_hbm, eu_hbm, ed_hbm, dg_hbm, du_hbm, dd_hbm = refs[:9]
    nbuf, out_ref = refs[9:11]
    held, refs = refs[11 : 11 + count], refs[11 + count :]
    (tokens_ref, gain_ref, doff_ref, coff_ref, cfac_ref, own_ref, hgain_ref, routes_ref,
     rweight_ref, wk_ref, wd_ref, wr_ref, wv_ref, wo_ref) = held
    (sbuf, pbuf, gather_ones, spread_ones, spread_in,
     eg, eu, ed, dg, du, dd, gain, goff, part_ref, hid_rows, p_in, xs, flat, hid, dens,
     ys, y_in, z_in, v_out, v_in, dg_in, d_out, d_in,
     arg_sem, in_sem,
     w_sem, s1, r1, st, rt, sc, rc, sa, ra, sb, rb, sv, rv, sg, rg, sd, rd) = refs
    f32, bf16 = jnp.float32, jnp.bfloat16
    zs = groups // 2
    me_g, me_l = lax.axis_index("ep"), lax.axis_index("tp")
    core, me_z = lax.rem(me_g, 2), me_g // 2
    partner = (me_g + 1 - 2 * core, me_l)

    side_x, side_y = lax.rem(me_l, 2), me_l // 2

    def lane_at(d):
        flip_x, flip_y = d % 2, d // 2
        x = side_x + flip_x - 2 * flip_x * side_x
        y = side_y + flip_y - 2 * flip_y * side_y
        return 2 * y + x

    def lane_peer(d):
        return (me_g, lane_at(d))

    def z_peer(d):
        return (lax.rem(me_z + d + zs, zs) * 2 + core, me_l)

    def send(src, dst, ssem, rsem, peer):
        copy = pltpu.make_async_remote_copy(
            src_ref=src, dst_ref=dst, send_sem=ssem, recv_sem=rsem, device_id=peer,
            device_id_type=pl.DeviceIdType.MESH,
        )
        copy.start()
        return copy

    seqs, width = tokens_ref.shape
    heads = state_ref.shape[1]
    rows = seqs // lanes
    args = [
        pltpu.make_async_copy(src, dst, arg_sem.at[i])
        for i, (src, dst) in enumerate(zip(sources, held))
    ]
    loads = [
        pltpu.make_async_copy(state_ref.at[:, h, :], sbuf.at[h], in_sem.at[h]) for h in range(heads)
    ]
    for arg in args[:-2]:
        arg.start()
    for load in loads:
        load.start()
    for arg in args[-2:]:
        arg.start()
    barrier = pltpu.get_barrier_semaphore()
    peers = [lane_peer(d) for d in range(1, lanes)] + [z_peer(d) for d in range(1, zs)] + [partner]
    for peer in peers:
        pl.semaphore_signal(barrier, inc=1, device_id=peer, device_id_type=pl.DeviceIdType.MESH)

    pair = 2 * HEAD_WIDTH
    flat_width = state_ref.shape[2]
    tile = 256

    offset = (
        lax.broadcasted_iota(jnp.int32, (tile, pair), 0) // HEAD_WIDTH
        - lax.broadcasted_iota(jnp.int32, (tile, pair), 1) % HEAD_WIDTH
    )
    for n in range(0, flat_width, tile):
        gather_ones[n : n + tile, :] = jnp.where(offset == -(n // HEAD_WIDTH), 1.0, 0.0).astype(bf16)

    half_r = lax.broadcasted_iota(jnp.int32, (pair, pair), 0) // HEAD_WIDTH
    half_c = lax.broadcasted_iota(jnp.int32, (pair, pair), 1) // HEAD_WIDTH
    ones_block = (half_r == half_c).astype(f32).astype(bf16)

    def group_sums(*blocks):
        parts = []
        for block in blocks:
            for i in range(0, block.shape[1], pair):
                piece = block[:, i : i + pair]
                high = piece.astype(bf16)
                parts += [high, (piece - high.astype(f32)).astype(bf16)]
        made = jnp.dot(jnp.concatenate(parts, axis=0), ones_block, preferred_element_type=f32)
        sums, at = [], 0
        for block in blocks:
            cols = []
            for i in range(0, block.shape[1], pair):
                cols.append(made[at : at + seqs] + made[at + seqs : at + 2 * seqs])
                at += 2 * seqs
            sums.append(jnp.concatenate(cols, axis=1))
        return sums

    lane = lax.broadcasted_iota(jnp.int32, (seqs, pair), 1)
    low = lane < HEAD_WIDTH

    def doubled(full, h):
        chunk = full[:, (h // 2) * pair : (h // 2 + 1) * pair]
        turned = pltpu.roll(chunk, HEAD_WIDTH, 1)
        return jnp.where(low, chunk, turned) if h % 2 == 0 else jnp.where(low, turned, chunk)

    for arg in args[:9]:
        arg.wait()
    toks = tokens_ref[...].astype(f32)
    normed = (
        toks * lax.rsqrt(jnp.mean(toks * toks, axis=-1, keepdims=True) + 1e-06) * gain_ref[...]
    ).astype(bf16)
    start = me_g * seqs + me_l * rows

    def picked_column(ref, k, first):
        spot = lax.broadcasted_iota(jnp.int32, (rows, ref.shape[1]), 1)
        wanted = spot == first + lax.broadcasted_iota(jnp.int32, spot.shape, 0)
        entries = ref[k : k + 1, :].astype(f32)
        return jnp.sum(jnp.where(wanted, entries, 0.0), axis=-1, keepdims=True)

    column = lax.broadcasted_iota(jnp.int32, (rows, 128), 1) % 64
    column = column.astype(f32)
    table = jnp.zeros((rows, 128), f32)
    for k in range(routes_ref.shape[0]):
        expert = picked_column(routes_ref, k, start)
        table = table + jnp.where(
            column == expert, picked_column(rweight_ref, k, me_l * rows), 0.0
        )
    high = table.astype(bf16).astype(f32)
    first_half = lax.broadcasted_iota(jnp.int32, table.shape, 1) < 64
    xs[0, 0, 0, :, width:] = jnp.where(first_half, high, table - high).astype(bf16)

    args[9].wait()
    keys = jnp.dot(normed, wk_ref[...], preferred_element_type=f32)
    args[10].wait()
    logits = jnp.dot(normed, wd_ref[...], preferred_element_type=f32)
    args[11].wait()
    recept = jnp.dot(normed, wr_ref[...], preferred_element_type=f32)
    for load in loads:
        load.wait()
    args[12].wait()
    values = jnp.dot(normed, wv_ref[...], preferred_element_type=f32)
    (key_squares,) = group_sums(keys * keys)
    rate = jax.nn.sigmoid(coff_ref[...] + cfac_ref[...] * keys)
    unit = keys * lax.rsqrt(key_squares * (1.0 / HEAD_WIDTH) + 1e-06) * HEAD_WIDTH ** (-0.5)
    key_in = keys * rate
    back = unit * rate
    decay = jnp.exp(-jnp.exp(doff_ref[...] + logits))
    faded = decay * recept
    back_sum, in_sum, own_sum = group_sums(
        back * recept, key_in * recept, recept * key_in * own_ref[...]
    )
    for h in range(heads):
        u2, f2 = doubled(unit, h), doubled(faded, h)
        for j in range(0, flat_width, pair):
            old = sbuf[h, :, j : j + pair]
            pbuf[2 * h * seqs : (2 * h + 1) * seqs, j : j + pair] = (old * u2).astype(bf16)
            pbuf[(2 * h + 1) * seqs : (2 * h + 2) * seqs, j : j + pair] = (old * f2).astype(bf16)
    sums = jnp.dot(pbuf[...], gather_ones[...], preferred_element_type=f32)

    def merged(first):
        picks = [sums[(2 * h + first) * seqs : (2 * h + first + 1) * seqs] for h in range(heads)]
        return jnp.concatenate(
            [jnp.where(low, picks[h], picks[h + 1]) for h in range(0, heads, 2)], axis=1
        )

    read = merged(1) - merged(0) * back_sum + values * in_sum
    (read_sum,) = group_sums(read)
    center = read - read_sum * (1.0 / HEAD_WIDTH)
    (square_sum,) = group_sums(center * center)
    heads_out = (
        center * lax.rsqrt(square_sum * (1.0 / HEAD_WIDTH) + 0.00064) * hgain_ref[...]
        + own_sum * values
    ).astype(bf16)
    args[13].wait()
    part = jnp.dot(heads_out, wo_ref[...], preferred_element_type=f32)
    base = jnp.zeros((rows, width), f32)
    for i in range(lanes):
        mine = part[i * rows : (i + 1) * rows]
        part_ref[i] = mine.astype(bf16)
        base = jnp.where(me_l == i, mine + toks[i * rows : (i + 1) * rows], base)
    hid_rows[...] = base
    pl.semaphore_wait(barrier, len(peers))
    sent = []
    firsts = []
    across = lanes - 1
    for d in (across, 1, 2):
        firsts.append(
            send(
                part_ref.at[lane_at(d)], p_in.at[d - 1], s1.at[d - 1], r1.at[d - 1], lane_peer(d)
            )
        )
    pulls = [
        pltpu.make_async_copy(src, dst, w_sem.at[i])
        for i, (src, dst) in enumerate(
            [(gain_hbm, gain), (goff_hbm, goff), (dg_hbm, dg), (du_hbm, du), (dd_hbm, dd),
             (eg_hbm.at[0], eg), (eu_hbm.at[0], eu), (ed_hbm.at[0], ed)]
        )
    ]
    for pull in pulls:
        pull.start()

    offset = (
        lax.broadcasted_iota(jnp.int32, (pair, tile), 0) % HEAD_WIDTH
        - lax.broadcasted_iota(jnp.int32, (pair, tile), 1) // HEAD_WIDTH
    )
    for n in range(0, flat_width, tile):
        spread_ones[:, n : n + tile] = jnp.where(offset == n // HEAD_WIDTH, 1.0, 0.0).astype(bf16)

    def halves(block):
        high = block.astype(bf16).astype(f32)
        return jnp.where(low, high, block - high).astype(bf16)

    for h in range(heads):
        spread_in[2 * h * seqs : (2 * h + 1) * seqs] = halves(
            sums[2 * h * seqs : (2 * h + 1) * seqs]
        )
        spread_in[(2 * h + 1) * seqs : (2 * h + 2) * seqs] = halves(doubled(values, h))
    fades = [doubled(decay, h) for h in range(heads)]
    backs = [doubled(back, h) for h in range(heads)]
    ins = [doubled(key_in, h) for h in range(heads)]
    for n in range(0, flat_width, tile):
        wide_rows = jnp.dot(
            spread_in[...], spread_ones[:, n : n + tile], preferred_element_type=f32
        )
        for h in range(heads):
            gone = wide_rows[2 * h * seqs : (2 * h + 1) * seqs]
            came = wide_rows[(2 * h + 1) * seqs : (2 * h + 2) * seqs]
            for i in range(0, tile, pair):
                nbuf[h, :, n + i : n + i + pair] = (
                    sbuf[h, :, n + i : n + i + pair] * fades[h]
                    - gone[:, i : i + pair] * backs[h]
                    + came[:, i : i + pair] * ins[h]
                )
    hidden = hid_rows[...]
    for copy in firsts:
        copy.wait_recv()
    for d in range(1, lanes):
        hidden = hidden + p_in[d - 1].astype(f32)
    sent += firsts
    hid_rows[...] = hidden
    for pull in pulls[:2]:
        pull.wait()
    normed = hidden * lax.rsqrt(jnp.mean(hidden * hidden, axis=-1, keepdims=True) + 1e-06)
    xs[0, 0, 0, :, :width] = (normed * gain[...]).astype(bf16)
    hold = {}

    def pass_block(d, q, to_d, to_q, peer):
        i = to_d * zs + to_q
        hold[to_d, to_q] = send(xs.at[0, d, q], xs.at[0, to_d, to_q], st.at[i], rt.at[i], peer)

    hold_c = {}

    def to_partner(d, q):
        i = d * zs + q
        hold_c[d, q] = send(xs.at[0, d, q], xs.at[1, d, q], sc.at[i], rc.at[i], partner)

    pass_block(0, 0, across, 0, lane_peer(across))
    for q in range(1, zs):
        pass_block(0, 0, 0, q, z_peer(q))
    for d in (1, 2):
        pass_block(0, 0, d, 0, lane_peer(d))
    to_partner(0, 0)

    def spread_row(q):
        hold[0, q].wait_recv()
        for d in (1, 2):
            pass_block(0, q, d, q, lane_peer(d))
        to_partner(0, q)

    spread_row(1)
    hold[across, 0].wait_recv()
    for q in range(1, zs):
        pass_block(across, 0, across, q, z_peer(q))
    for q in range(2, zs):
        spread_row(q)
    to_partner(across, 0)
    for d in (1, 2):
        hold[d, 0].wait_recv()
        to_partner(d, 0)
    block = 2 * zs * rows

    def gathered(d):
        return xs[:, d].astype(f32).reshape(block, width + 128)

    for q in range(zs):
        hold_c[0, q].wait_recv()
    mine = gathered(0)
    flat[0:block] = mine.astype(bf16)
    own_rows = mine[:, :width].astype(bf16)
    for pull in pulls[2:5]:
        pull.wait()
    turned = (((1,), (1,)), ((), ()))
    gate = lax.dot_general(own_rows, dg[...], turned, preferred_element_type=f32)
    up = lax.dot_general(own_rows, du[...], turned, preferred_element_type=f32)
    mixed = (jax.nn.silu(gate) * up).astype(bf16)
    dens[...] = jnp.dot(mixed, dd[...], preferred_element_type=f32) * jax.nn.sigmoid(goff[...])
    for q in range(1, zs):
        for d in range(1, lanes):
            hold[d, q].wait_recv()
            to_partner(d, q)
    for d in range(1, lanes):
        for q in range(zs):
            hold_c[d, q].wait_recv()
        flat[d * block : (d + 1) * block] = gathered(d).astype(bf16)
    for pull in pulls[5:]:
        pull.wait()

    @pl.loop(0, eg.shape[1] // tile, unroll=True)
    def _(n):
        cols = pl.ds(pl.multiple_of(n * tile, tile), tile)
        left = flat[:, :width]
        gated = jnp.dot(left, eg[:, cols], preferred_element_type=f32)
        raised = jnp.dot(left, eu[:, cols], preferred_element_type=f32)
        hid[:, cols] = (jax.nn.silu(gated) * raised).astype(bf16)

    tail = flat[:, width:].astype(f32)
    picked = lax.broadcasted_iota(jnp.int32, tail.shape, 1) % 64 == me_g
    scale = jnp.sum(jnp.where(picked, tail, 0.0), axis=-1, keepdims=True)
    pieces, wide = ys.shape[0], ys.shape[-1]
    to_core, to_lane, to_diag, to_last, to_z = [], [], [], [], []

    def pass_on(n):
        to_core[n].wait_recv()
        own = []
        for q in range(1, zs):
            i = n * (zs - 1) + q - 1
            ys[n, 0, across, q] = (
                ys[n, 0, across, q].astype(f32) + y_in[n, across, q].astype(f32)
            ).astype(bf16)
            own.append(
                send(ys.at[n, 0, across, q], dg_in.at[n, q - 1], sg.at[i], rg.at[i], z_peer(-q))
            )
        to_diag.append(own)
        own = []
        for d in (1, 2):
            ys[n, 0, d] = (ys[n, 0, d].astype(f32) + y_in[n, d].astype(f32)).astype(bf16)
            i = 2 * n + d - 1
            own.append(
                send(ys.at[n, 0, d], z_in.at[n, d - 1], sb.at[i], rb.at[i], lane_peer(d))
            )
        to_lane.append(own)

    for n in range(pieces):
        cols = slice(n * wide, (n + 1) * wide)
        made = jnp.dot(hid[...], ed[:, cols], preferred_element_type=f32) * scale
        for d in range(lanes):
            piece = made[d * block : (d + 1) * block]
            if d == 0:
                piece = piece + dens[:, cols]
            ys[n, :, d] = piece.reshape(2, zs, rows, wide).astype(bf16)
        to_core.append(send(ys.at[n, 1], y_in.at[n], sa.at[n], ra.at[n], partner))
        if n > 0:
            pass_on(n - 1)
    pass_on(pieces - 1)
    for n in range(pieces):
        cols = slice(n * wide, (n + 1) * wide)
        total = ys[n, 0, across, 0].astype(f32) + y_in[n, across, 0].astype(f32)
        for q in range(1, zs):
            to_diag[n][q - 1].wait_recv()
            total = total + dg_in[n, q - 1].astype(f32)
        d_out[n] = total.astype(bf16)
        to_last.append(send(d_out.at[n], d_in.at[n], sd.at[n], rd.at[n], lane_peer(across)))
        total = ys[n, 0, 0].astype(f32) + y_in[n, 0].astype(f32)
        for d in (1, 2):
            to_lane[n][d - 1].wait_recv()
            total = total + z_in[n, d - 1].astype(f32)
        v_out[n] = total.astype(bf16)
        own = []
        for q in range(1, zs):
            i = n * (zs - 1) + q - 1
            own.append(
                send(v_out.at[n, q], v_in.at[n, q - 1], sv.at[i], rv.at[i], z_peer(-q))
            )
        to_z.append(own)
        hid_rows[:, cols] = hid_rows[:, cols] + total[0]
    for n in range(pieces):
        cols = slice(n * wide, (n + 1) * wide)
        result = hid_rows[:, cols]
        to_last[n].wait_recv()
        result = result + d_in[n].astype(f32)
        for d, copy in enumerate(to_z[n]):
            copy.wait_recv()
            result = result + v_in[n, d].astype(f32)
        out_ref[:, cols] = result.astype(bf16)
    sent += list(hold.values()) + list(hold_c.values())
    sent += to_core + to_last
    for own in to_lane + to_diag + to_z:
        sent += own
    for copy in sent:
        copy.wait_send()


def hand_over_kernel(rows_ref, state_ref, out_ref, next_ref, row_sem, state_sem):
    heads = state_ref.shape[0]
    copies = [pltpu.make_async_copy(rows_ref, out_ref, row_sem)] + [
        pltpu.make_async_copy(state_ref.at[h], next_ref.at[:, h, :], state_sem.at[h])
        for h in range(heads)
    ]
    for copy in copies:
        copy.start()
    for copy in copies:
        copy.wait()


def fused(
    tokens, recurrent_head_state, first_norm_gain, receptance_matrix, key_matrix, value_matrix,
    decay_matrix, decay_offset, correction_offset, correction_key_factor, own_term_weight,
    head_norm_gain, output_matrix, second_norm_gain, routing, routing_weight, expert_gate_weight,
    expert_up_weight, expert_down_weight, dense_gate_weight, dense_up_weight, dense_down_weight,
    dense_gate_offset,
):
    f32, bf16 = jnp.float32, jnp.bfloat16
    seqs, width = tokens.shape
    heads, flat_width = recurrent_head_state.shape[1:]
    groups, lanes = lax.axis_size("ep"), lax.axis_size("tp")
    rows, zs = seqs // lanes, groups // 2
    grant = VMEM_BYTES - rows * width * 2 - heads * seqs * flat_width * 4
    vmem = pl.BlockSpec(memory_space=pltpu.VMEM)
    anywhere = pl.BlockSpec(memory_space=pltpu.HBM)
    dma = pltpu.SemaphoreType.DMA

    def row(vector):
        return vector.reshape(1, -1)

    operands = (
        tokens, row(first_norm_gain), row(decay_offset), row(correction_offset),
        row(correction_key_factor), row(own_term_weight), row(head_norm_gain), routing.T,
        routing_weight.T, key_matrix, decay_matrix, receptance_matrix, value_matrix, output_matrix,
    )
    count = len(operands)
    hidden_units = expert_gate_weight.shape[2]
    pieces = 4
    wide = width // pieces
    total = groups * seqs
    pair = 2 * HEAD_WIDTH
    next_state, layer_rows = pl.pallas_call(
        functools.partial(fused_kernel, count, groups, lanes),
        out_shape=(
            pltpu.VMEM((heads, seqs, flat_width), f32),
            pltpu.VMEM((rows, width), bf16),
        ),
        in_specs=[anywhere] * (count + 9),
        out_specs=(vmem, vmem),
        scratch_shapes=[pltpu.VMEM(operand.shape, operand.dtype) for operand in operands]
        + [
            pltpu.VMEM((heads, seqs, flat_width), f32),
            pltpu.VMEM((2 * heads * seqs, flat_width), bf16),
            pltpu.VMEM((flat_width, pair), bf16),
            pltpu.VMEM((pair, flat_width), bf16),
            pltpu.VMEM((2 * heads * seqs, pair), bf16),
            pltpu.VMEM(expert_gate_weight.shape[1:], bf16),
            pltpu.VMEM(expert_up_weight.shape[1:], bf16),
            pltpu.VMEM(expert_down_weight.shape[1:], bf16),
            pltpu.VMEM(dense_gate_weight.shape[::-1], bf16),
            pltpu.VMEM(dense_up_weight.shape[::-1], bf16),
            pltpu.VMEM(dense_down_weight.shape, bf16),
            pltpu.VMEM((1, width), f32),
            pltpu.VMEM((1, width), f32),
            pltpu.VMEM((lanes, rows, width), bf16),
            pltpu.VMEM((rows, width), f32),
            pltpu.VMEM((lanes - 1, rows, width), bf16),
            pltpu.VMEM((2, lanes, zs, rows, width + 128), bf16),
            pltpu.VMEM((total, width + 128), bf16),
            pltpu.VMEM((total, hidden_units), bf16),
            pltpu.VMEM((2 * zs * rows, width), f32),
            pltpu.VMEM((pieces, 2, lanes, zs, rows, wide), bf16),
            pltpu.VMEM((pieces, lanes, zs, rows, wide), bf16),
            pltpu.VMEM((pieces, 2, zs, rows, wide), bf16),
            pltpu.VMEM((pieces, zs, rows, wide), bf16),
            pltpu.VMEM((pieces, zs - 1, rows, wide), bf16),
            pltpu.VMEM((pieces, zs - 1, rows, wide), bf16),
            pltpu.VMEM((pieces, rows, wide), bf16),
            pltpu.VMEM((pieces, rows, wide), bf16),
            dma((count,)),
            dma((heads,)),
            dma((8,)),
            dma((lanes - 1,)), dma((lanes - 1,)),
            dma((lanes * zs,)), dma((lanes * zs,)),
            dma((lanes * zs,)), dma((lanes * zs,)),
            dma((pieces,)), dma((pieces,)),
            dma((pieces * 2,)), dma((pieces * 2,)),
            dma((pieces * (zs - 1),)), dma((pieces * (zs - 1),)),
            dma((pieces * (zs - 1),)), dma((pieces * (zs - 1),)),
            dma((pieces,)), dma((pieces,)),
        ],
        compiler_params=pltpu.CompilerParams(
            collective_id=0, has_side_effects=True, vmem_limit_bytes=grant
        ),
        name="layer",
    )(
        *operands, recurrent_head_state, row(second_norm_gain), row(dense_gate_offset),
        expert_gate_weight, expert_up_weight, expert_down_weight, dense_gate_weight.T,
        dense_up_weight.T, dense_down_weight,
    )
    return pl.pallas_call(
        hand_over_kernel,
        out_shape=(
            jax.ShapeDtypeStruct((rows, width), bf16),
            jax.ShapeDtypeStruct(recurrent_head_state.shape, f32),
        ),
        in_specs=[vmem, vmem],
        out_specs=(anywhere, anywhere),
        scratch_shapes=[dma, dma((heads,))],
        compiler_params=pltpu.CompilerParams(vmem_limit_bytes=1 << 20),
        name="hand_over",
    )(
        pltpu.with_memory_space_constraint(layer_rows, pltpu.VMEM),
        pltpu.with_memory_space_constraint(next_state, pltpu.VMEM),
    )


def choose(tokens, recurrent_head_state, *rest):
    groups, lanes = lax.axis_size("ep"), lax.axis_size("tp")
    rows, heads = tokens.shape[0] // lanes, recurrent_head_state.shape[1]
    experts_here = rest[14].shape[0]
    fits = (
        rows % 8 == 0 and heads % 2 == 0 and groups % 2 == 0 and groups > 2 and lanes == 4
        and groups <= 64 and experts_here == 1
    )
    return (fused if fits else local)(tokens, recurrent_head_state, *rest)


def solution(mesh):
    return jax.shard_map(
        choose,
        mesh=mesh,
        in_specs=(
            P("ep", None),
            P("ep", "tp", None),
            P(),
            P(None, "tp"),
            P(None, "tp"),
            P(None, "tp"),
            P(None, "tp"),
            P("tp"),
            P("tp"),
            P("tp"),
            P("tp"),
            P("tp"),
            P("tp", None),
            P(),
            P(),
            P("ep", None),
            P("ep", None, "tp"),
            P("ep", None, "tp"),
            P("ep", "tp", None),
            P(None, "ep"),
            P(None, "ep"),
            P("ep", None),
            P(),
        ),
        out_specs=(P(("ep", "tp"), None), P("ep", "tp", None)),
        check_vma=False,
    )
```

```python
import functools

import jax
import jax.numpy as jnp
from jax import lax
from jax.experimental import pallas as pl
from jax.experimental.pallas import tpu as pltpu
from jax.sharding import PartitionSpec as P

HEAD_WIDTH = 64
VMEM_BYTES = 67043328


PRECISE = lax.Precision.HIGHEST


def rms_scale(rows, gain):
    floats = rows.astype(jnp.float32)
    return floats * lax.rsqrt(jnp.mean(floats * floats, axis=-1, keepdims=True) + 1e-06) * gain


def route_table(block_routes, experts, capacity):
    flat_routes = block_routes.reshape(-1)
    chosen = (flat_routes[:, None] == jnp.arange(experts, dtype=jnp.int32)[None, :]).astype(
        jnp.int32
    )
    before = jnp.cumsum(chosen, axis=0, dtype=jnp.int32) - chosen
    slot_index = jnp.sum(before * chosen, axis=1)
    slot_match = (slot_index[:, None] == jnp.arange(capacity, dtype=jnp.int32)[None, :]).astype(
        jnp.float32
    )
    dispatch_table = chosen.astype(jnp.float32)[:, :, None] * slot_match[:, None, :]
    return dispatch_table.reshape(block_routes.shape[0], block_routes.shape[1], experts, capacity)


def state_update(
    receptance_rows,
    key_matrix_rows,
    value_matrix_rows,
    decay_logits,
    recurrent_head_state,
    decay_offset,
    correction_offset,
    correction_key_factor,
    own_term_weight,
    head_norm_gain,
    head_width,
):
    seq_count = key_matrix_rows.shape[0]
    decay_factor = jnp.exp(-jnp.exp(decay_offset + decay_logits))
    in_rate = jax.nn.sigmoid(correction_offset + correction_key_factor * key_matrix_rows)
    key_in = key_matrix_rows * in_rate

    def split_heads(block):
        return block.reshape(seq_count, -1, head_width)

    keys_head = split_heads(key_matrix_rows)
    unit_keys = (
        keys_head
        * lax.rsqrt(jnp.mean(keys_head * keys_head, axis=-1, keepdims=True) + 1e-06)
        * head_width ** (-0.5)
    )
    rate_head = split_heads(in_rate)
    head_keys = split_heads(key_in)
    decay_head = split_heads(decay_factor)
    head_values = split_heads(value_matrix_rows)
    head_receptance = split_heads(receptance_rows)
    matrix = recurrent_head_state.reshape(seq_count, -1, head_width, head_width)
    removed = jnp.einsum("bhvk,bhk->bhv", matrix, unit_keys, precision=PRECISE)
    updated = (
        matrix * decay_head[:, :, None, :]
        - removed[..., None] * (unit_keys * rate_head)[:, :, None, :]
        + head_values[..., None] * head_keys[:, :, None, :]
    )
    readout = jnp.einsum("bhvk,bhk->bhv", updated, head_receptance, precision=PRECISE)
    center = jnp.mean(readout, axis=-1, keepdims=True)
    spread = jnp.mean(jnp.square(readout - center), axis=-1, keepdims=True)
    normalized_rows = (
        (readout - center) * lax.rsqrt(spread + 0.00064) * head_norm_gain.reshape(-1, head_width)
    )
    own_term_total = jnp.sum(
        head_receptance * head_keys * own_term_weight.reshape(-1, head_width),
        axis=-1,
        keepdims=True,
    )
    normalized_rows = normalized_rows + own_term_total * head_values
    return (
        normalized_rows.reshape(seq_count, -1).astype(jnp.bfloat16),
        updated.reshape(seq_count, -1, head_width * head_width),
    )


def local(
    tokens,
    recurrent_head_state,
    first_norm_gain,
    receptance_matrix,
    key_matrix,
    value_matrix,
    decay_matrix,
    decay_offset,
    correction_offset,
    correction_key_factor,
    own_term_weight,
    head_norm_gain,
    output_matrix,
    second_norm_gain,
    routing,
    routing_weight,
    expert_gate_weight,
    expert_up_weight,
    expert_down_weight,
    dense_gate_weight,
    dense_up_weight,
    dense_down_weight,
    dense_gate_offset,
):
    seq_count = tokens.shape[0]
    width = tokens.shape[1]
    group_index = lax.axis_index("ep")
    lane_index = lax.axis_index("tp")
    group_count = lax.axis_size("ep")
    lane_count = lax.axis_size("tp")
    normalized_rows = rms_scale(tokens, first_norm_gain).astype(jnp.bfloat16)
    receptance_rows = jnp.dot(
        normalized_rows, receptance_matrix, preferred_element_type=jnp.float32
    )
    key_matrix_rows = jnp.dot(normalized_rows, key_matrix, preferred_element_type=jnp.float32)
    value_matrix_rows = jnp.dot(normalized_rows, value_matrix, preferred_element_type=jnp.float32)
    decay_logits = jnp.dot(normalized_rows, decay_matrix, preferred_element_type=jnp.float32)
    head_outputs, next_state = state_update(
        receptance_rows,
        key_matrix_rows,
        value_matrix_rows,
        decay_logits,
        recurrent_head_state,
        decay_offset,
        correction_offset,
        correction_key_factor,
        own_term_weight,
        head_norm_gain,
        HEAD_WIDTH,
    )
    partial_out = jnp.dot(head_outputs, output_matrix, preferred_element_type=jnp.float32)
    hidden_sum = tokens.astype(jnp.float32) + lax.psum(
        partial_out.astype(jnp.bfloat16), "tp"
    ).astype(jnp.float32)
    ffn_in = rms_scale(hidden_sum, second_norm_gain).astype(jnp.bfloat16)
    local_experts = expert_gate_weight.shape[0]
    top_count = routing.shape[1]
    expert_count = local_experts * group_count
    capacity = 2 * seq_count * top_count // expert_count
    per_lane = seq_count // lane_count
    own_routes = lax.dynamic_slice_in_dim(routing, group_index * seq_count, seq_count, 0)
    own_table = route_table(own_routes, expert_count, capacity)
    send_rows = jnp.einsum(
        "bkec,bd->ecd", own_table.astype(jnp.bfloat16), ffn_in, preferred_element_type=jnp.float32
    ).astype(jnp.bfloat16)
    lane_rows = lax.dynamic_slice_in_dim(ffn_in, lane_index * per_lane, per_lane, 0)
    dense_send = jnp.broadcast_to(lane_rows[None], (group_count, per_lane, width))
    expert_in, dense_in = (
        lax.all_to_all(send_rows, "ep", split_axis=0, concat_axis=0, tiled=True),
        lax.all_to_all(dense_send, "ep", split_axis=0, concat_axis=0, tiled=True),
    )
    rows_in = expert_in.reshape(group_count, local_experts, capacity, width).transpose(1, 0, 2, 3)
    rows_in = rows_in.reshape(local_experts, group_count * capacity, width)
    gate_pre = jnp.einsum(
        "lrd,ldf->lrf", rows_in, expert_gate_weight, preferred_element_type=jnp.float32
    )
    up_pre = jnp.einsum(
        "lrd,ldf->lrf", rows_in, expert_up_weight, preferred_element_type=jnp.float32
    )
    expert_hidden = (jax.nn.silu(gate_pre) * up_pre).astype(jnp.bfloat16)
    expert_part = jnp.einsum(
        "lrf,lfd->lrd", expert_hidden, expert_down_weight, preferred_element_type=jnp.float32
    )
    expert_out = lax.psum_scatter(
        expert_part.astype(jnp.bfloat16), "tp", scatter_dimension=2, tiled=True
    )
    back_send = expert_out.reshape(local_experts, group_count, capacity, -1).transpose(1, 0, 2, 3)
    back_send = back_send.reshape(group_count * local_experts, capacity, -1)
    dense_rows = dense_in.reshape(group_count * per_lane, width)
    dense_hidden = (
        jax.nn.silu(jnp.dot(dense_rows, dense_gate_weight, preferred_element_type=jnp.float32))
        * jnp.dot(dense_rows, dense_up_weight, preferred_element_type=jnp.float32)
    ).astype(jnp.bfloat16)
    dense_part = jnp.dot(
        dense_hidden, dense_down_weight, preferred_element_type=jnp.float32
    ).astype(jnp.bfloat16)
    dense_part = dense_part.reshape(group_count, per_lane, width)
    back_experts, back_dense = (
        lax.all_to_all(back_send, "ep", split_axis=0, concat_axis=0, tiled=True),
        lax.all_to_all(dense_part, "ep", split_axis=0, concat_axis=0, tiled=True),
    )
    dense_sum = jnp.sum(back_dense.astype(jnp.float32), axis=0)
    weighted = jnp.einsum("bkec,bk->ecb", own_table, routing_weight, precision=PRECISE)
    moe_slice = jnp.einsum(
        "ecb,ecd->bd", weighted, back_experts.astype(jnp.float32), precision=PRECISE
    )
    moe_rows = lax.all_to_all(moe_slice, "tp", split_axis=0, concat_axis=1, tiled=True)
    residual_rows = lax.dynamic_slice_in_dim(hidden_sum, lane_index * per_lane, per_lane, 0)
    layer_out = (residual_rows + moe_rows + jax.nn.sigmoid(dense_gate_offset) * dense_sum).astype(
        jnp.bfloat16
    )
    return (layer_out, next_state)


def fused_kernel(count, groups, lanes, *refs):
    sources, refs = refs[:count], refs[count:]
    state_ref, gain_hbm, goff_hbm, eg_hbm, eu_hbm, ed_hbm, dg_hbm, du_hbm, dd_hbm = refs[:9]
    nbuf, out_ref = refs[9:11]
    held, refs = refs[11 : 11 + count], refs[11 + count :]
    (tokens_ref, gain_ref, doff_ref, coff_ref, cfac_ref, own_ref, hgain_ref, routes_ref,
     rweight_ref, wk_ref, wd_ref, wr_ref, wv_ref, wo_ref) = held
    (sbuf, pbuf, gather_ones, spread_ones, spread_in,
     eg, eu, ed, dg, du, dd, gain, goff, part_ref, hid_rows, p_in, xs, flat, hid, dens,
     ys, y_in, z_in, v_out, v_in, dg_in, d_out, d_in,
     arg_sem, in_sem,
     w_sem, s1, r1, st, rt, sc, rc, sa, ra, sb, rb, sv, rv, sg, rg, sd, rd) = refs
    f32, bf16 = jnp.float32, jnp.bfloat16
    zs = groups // 2
    me_g, me_l = lax.axis_index("ep"), lax.axis_index("tp")
    core, me_z = lax.rem(me_g, 2), me_g // 2
    partner = (me_g + 1 - 2 * core, me_l)

    side_x, side_y = lax.rem(me_l, 2), me_l // 2

    def lane_at(d):
        flip_x, flip_y = d % 2, d // 2
        x = side_x + flip_x - 2 * flip_x * side_x
        y = side_y + flip_y - 2 * flip_y * side_y
        return 2 * y + x

    def lane_peer(d):
        return (me_g, lane_at(d))

    def far_lane(d):
        return (partner[0], lane_at(d))

    def far_z(d):
        return (lax.rem(me_z + d + zs, zs) * 2 + 1 - core, me_l)

    def send(src, dst, ssem, rsem, peer):
        copy = pltpu.make_async_remote_copy(
            src_ref=src, dst_ref=dst, send_sem=ssem, recv_sem=rsem, device_id=peer,
            device_id_type=pl.DeviceIdType.MESH,
        )
        copy.start()
        return copy

    def whole(ref, sem):
        return pltpu.make_async_remote_copy(
            src_ref=ref, dst_ref=ref, send_sem=sem, recv_sem=sem, device_id=partner,
            device_id_type=pl.DeviceIdType.MESH,
        )

    seqs, width = tokens_ref.shape
    heads = state_ref.shape[1]
    rows = seqs // lanes
    args = [
        pltpu.make_async_copy(src, dst, arg_sem.at[i])
        for i, (src, dst) in enumerate(zip(sources, held))
    ]
    loads = [
        pltpu.make_async_copy(state_ref.at[:, h, :], sbuf.at[h], in_sem.at[h]) for h in range(heads)
    ]
    for arg in args[:-2]:
        arg.start()
    for load in loads:
        load.start()
    for arg in args[-2:]:
        arg.start()
    barrier = pltpu.get_barrier_semaphore()
    peers = [lane_peer(d) for d in range(1, lanes)] + [far_lane(d) for d in range(1, lanes)]
    peers += [far_z(d) for d in range(1, zs)] + [partner]
    for peer in peers:
        pl.semaphore_signal(barrier, inc=1, device_id=peer, device_id_type=pl.DeviceIdType.MESH)

    pair = 2 * HEAD_WIDTH
    flat_width = state_ref.shape[2]
    tile = 256

    offset = (
        lax.broadcasted_iota(jnp.int32, (tile, pair), 0) // HEAD_WIDTH
        - lax.broadcasted_iota(jnp.int32, (tile, pair), 1) % HEAD_WIDTH
    )
    for n in range(0, flat_width, tile):
        gather_ones[n : n + tile, :] = jnp.where(offset == -(n // HEAD_WIDTH), 1.0, 0.0).astype(bf16)

    half_r = lax.broadcasted_iota(jnp.int32, (pair, pair), 0) // HEAD_WIDTH
    half_c = lax.broadcasted_iota(jnp.int32, (pair, pair), 1) // HEAD_WIDTH
    ones_block = (half_r == half_c).astype(f32).astype(bf16)

    def group_sums(*blocks):
        parts = []
        for block in blocks:
            for i in range(0, block.shape[1], pair):
                piece = block[:, i : i + pair]
                high = piece.astype(bf16)
                parts += [high, (piece - high.astype(f32)).astype(bf16)]
        made = jnp.dot(jnp.concatenate(parts, axis=0), ones_block, preferred_element_type=f32)
        sums, at = [], 0
        for block in blocks:
            cols = []
            for i in range(0, block.shape[1], pair):
                cols.append(made[at : at + seqs] + made[at + seqs : at + 2 * seqs])
                at += 2 * seqs
            sums.append(jnp.concatenate(cols, axis=1))
        return sums

    lane = lax.broadcasted_iota(jnp.int32, (seqs, pair), 1)
    low = lane < HEAD_WIDTH

    def doubled(full, h):
        chunk = full[:, (h // 2) * pair : (h // 2 + 1) * pair]
        turned = pltpu.roll(chunk, HEAD_WIDTH, 1)
        return jnp.where(low, chunk, turned) if h % 2 == 0 else jnp.where(low, turned, chunk)

    for arg in args[:9]:
        arg.wait()
    toks = tokens_ref[...].astype(f32)
    normed = (
        toks * lax.rsqrt(jnp.mean(toks * toks, axis=-1, keepdims=True) + 1e-06) * gain_ref[...]
    ).astype(bf16)
    start = me_g * seqs + me_l * rows

    def picked_column(ref, k, first):
        spot = lax.broadcasted_iota(jnp.int32, (rows, ref.shape[1]), 1)
        wanted = spot == first + lax.broadcasted_iota(jnp.int32, spot.shape, 0)
        entries = ref[k : k + 1, :].astype(f32)
        return jnp.sum(jnp.where(wanted, entries, 0.0), axis=-1, keepdims=True)

    column = lax.broadcasted_iota(jnp.int32, (rows, 128), 1) % 64
    column = column.astype(f32)
    table = jnp.zeros((rows, 128), f32)
    for k in range(routes_ref.shape[0]):
        expert = picked_column(routes_ref, k, start)
        table = table + jnp.where(
            column == expert, picked_column(rweight_ref, k, me_l * rows), 0.0
        )
    high = table.astype(bf16).astype(f32)
    first_half = lax.broadcasted_iota(jnp.int32, table.shape, 1) < 64
    xs[0, 0, 0, :, width:] = jnp.where(first_half, high, table - high).astype(bf16)

    args[9].wait()
    keys = jnp.dot(normed, wk_ref[...], preferred_element_type=f32)
    args[10].wait()
    logits = jnp.dot(normed, wd_ref[...], preferred_element_type=f32)
    args[11].wait()
    recept = jnp.dot(normed, wr_ref[...], preferred_element_type=f32)
    for load in loads:
        load.wait()
    args[12].wait()
    values = jnp.dot(normed, wv_ref[...], preferred_element_type=f32)
    (key_squares,) = group_sums(keys * keys)
    rate = jax.nn.sigmoid(coff_ref[...] + cfac_ref[...] * keys)
    unit = keys * lax.rsqrt(key_squares * (1.0 / HEAD_WIDTH) + 1e-06) * HEAD_WIDTH ** (-0.5)
    key_in = keys * rate
    back = unit * rate
    decay = jnp.exp(-jnp.exp(doff_ref[...] + logits))
    faded = decay * recept
    back_sum, in_sum, own_sum = group_sums(
        back * recept, key_in * recept, recept * key_in * own_ref[...]
    )
    for h in range(heads):
        u2, f2 = doubled(unit, h), doubled(faded, h)
        for j in range(0, flat_width, pair):
            old = sbuf[h, :, j : j + pair]
            pbuf[2 * h * seqs : (2 * h + 1) * seqs, j : j + pair] = (old * u2).astype(bf16)
            pbuf[(2 * h + 1) * seqs : (2 * h + 2) * seqs, j : j + pair] = (old * f2).astype(bf16)
    sums = jnp.dot(pbuf[...], gather_ones[...], preferred_element_type=f32)

    def merged(first):
        picks = [sums[(2 * h + first) * seqs : (2 * h + first + 1) * seqs] for h in range(heads)]
        return jnp.concatenate(
            [jnp.where(low, picks[h], picks[h + 1]) for h in range(0, heads, 2)], axis=1
        )

    read = merged(1) - merged(0) * back_sum + values * in_sum
    (read_sum,) = group_sums(read)
    center = read - read_sum * (1.0 / HEAD_WIDTH)
    (square_sum,) = group_sums(center * center)
    heads_out = (
        center * lax.rsqrt(square_sum * (1.0 / HEAD_WIDTH) + 0.00064) * hgain_ref[...]
        + own_sum * values
    ).astype(bf16)
    args[13].wait()
    part = jnp.dot(heads_out, wo_ref[...], preferred_element_type=f32)
    base = jnp.zeros((rows, width), f32)
    for i in range(lanes):
        mine = part[i * rows : (i + 1) * rows]
        part_ref[i] = mine.astype(bf16)
        base = jnp.where(me_l == i, mine + toks[i * rows : (i + 1) * rows], base)
    hid_rows[...] = base
    pl.semaphore_wait(barrier, len(peers))
    across = lanes - 1
    for d in (across, 1, 2):
        send(part_ref.at[lane_at(d)], p_in.at[d - 1], s1, r1, lane_peer(d))
    pulls = [
        pltpu.make_async_copy(src, dst, w_sem.at[i])
        for i, (src, dst) in enumerate(
            [(gain_hbm, gain), (goff_hbm, goff), (dg_hbm, dg), (du_hbm, du), (dd_hbm, dd),
             (eg_hbm.at[0], eg), (eu_hbm.at[0], eu), (ed_hbm.at[0], ed)]
        )
    ]
    for pull in pulls:
        pull.start()

    offset = (
        lax.broadcasted_iota(jnp.int32, (pair, tile), 0) % HEAD_WIDTH
        - lax.broadcasted_iota(jnp.int32, (pair, tile), 1) // HEAD_WIDTH
    )
    for n in range(0, flat_width, tile):
        spread_ones[:, n : n + tile] = jnp.where(offset == n // HEAD_WIDTH, 1.0, 0.0).astype(bf16)

    def halves(block):
        high = block.astype(bf16).astype(f32)
        return jnp.where(low, high, block - high).astype(bf16)

    for h in range(heads):
        spread_in[2 * h * seqs : (2 * h + 1) * seqs] = halves(
            sums[2 * h * seqs : (2 * h + 1) * seqs]
        )
        spread_in[(2 * h + 1) * seqs : (2 * h + 2) * seqs] = halves(doubled(values, h))
    fades = [doubled(decay, h) for h in range(heads)]
    backs = [doubled(back, h) for h in range(heads)]
    ins = [doubled(key_in, h) for h in range(heads)]
    for n in range(0, flat_width, tile):
        wide_rows = jnp.dot(
            spread_in[...], spread_ones[:, n : n + tile], preferred_element_type=f32
        )
        for h in range(heads):
            gone = wide_rows[2 * h * seqs : (2 * h + 1) * seqs]
            came = wide_rows[(2 * h + 1) * seqs : (2 * h + 2) * seqs]
            for i in range(0, tile, pair):
                nbuf[h, :, n + i : n + i + pair] = (
                    sbuf[h, :, n + i : n + i + pair] * fades[h]
                    - gone[:, i : i + pair] * backs[h]
                    + came[:, i : i + pair] * ins[h]
                )
    hidden = hid_rows[...]
    whole(p_in, r1).wait_recv()
    for d in range(1, lanes):
        hidden = hidden + p_in[d - 1].astype(f32)
    hid_rows[...] = hidden
    for pull in pulls[:2]:
        pull.wait()
    normed = hidden * lax.rsqrt(jnp.mean(hidden * hidden, axis=-1, keepdims=True) + 1e-06)
    xs[0, 0, 0, :, :width] = (normed * gain[...]).astype(bf16)
    hold = {}

    def pass_block(d, q, to_d, to_q, peer):
        hold[to_d, to_q] = send(
            xs.at[0, d, q], xs.at[0, to_d, to_q], st.at[0 if (d, q) == (0, 0) else 1],
            rt.at[to_d * zs + to_q], peer,
        )

    def to_partner(d, q):
        send(xs.at[0, d, q], xs.at[1, d, q], sc, rc.at[0 if d == 0 else 1], partner)

    pass_block(0, 0, across, 0, far_lane(across))
    for q in range(1, zs):
        pass_block(0, 0, 0, q, far_z(q))
    for d in (1, 2):
        pass_block(0, 0, d, 0, far_lane(d))
    to_partner(0, 0)

    def spread_row(q):
        hold[0, q].wait_recv()
        for d in (1, 2):
            pass_block(0, q, d, q, far_lane(d))
        to_partner(0, q)

    hold[across, 0].wait_recv()
    for q in range(1, zs):
        pass_block(across, 0, across, q, far_z(q))
    for q in range(zs - 1, 0, -1):
        spread_row(q)
    to_partner(across, 0)
    for d in (1, 2):
        hold[d, 0].wait_recv()
        to_partner(d, 0)
    block = 2 * zs * rows

    def gathered(d):
        return xs[:, d].astype(f32).reshape(block, width + 128)

    whole(xs.at[1, 0], rc.at[0]).wait_recv()
    mine = gathered(0)
    flat[0:block] = mine.astype(bf16)
    own_rows = mine[:, :width].astype(bf16)
    for pull in pulls[2:5]:
        pull.wait()
    turned = (((1,), (1,)), ((), ()))
    gate = lax.dot_general(own_rows, dg[...], turned, preferred_element_type=f32)
    up = lax.dot_general(own_rows, du[...], turned, preferred_element_type=f32)
    mixed = (jax.nn.silu(gate) * up).astype(bf16)
    dens[...] = jnp.dot(mixed, dd[...], preferred_element_type=f32) * jax.nn.sigmoid(goff[...])
    for q in range(zs - 1, 0, -1):
        for d in range(1, lanes):
            hold[d, q].wait_recv()
            to_partner(d, q)
    whole(xs.at[1, 1:], rc.at[1]).wait_recv()
    for d in range(1, lanes):
        flat[d * block : (d + 1) * block] = gathered(d).astype(bf16)
    for pull in pulls[5:]:
        pull.wait()

    @pl.loop(0, eg.shape[1] // tile, unroll=True)
    def _(n):
        cols = pl.ds(pl.multiple_of(n * tile, tile), tile)
        left = flat[:, :width]
        gated = jnp.dot(left, eg[:, cols], preferred_element_type=f32)
        raised = jnp.dot(left, eu[:, cols], preferred_element_type=f32)
        hid[:, cols] = (jax.nn.silu(gated) * raised).astype(bf16)

    tail = flat[:, width:].astype(f32)
    picked = lax.broadcasted_iota(jnp.int32, tail.shape, 1) % 64 == me_g
    scale = jnp.sum(jnp.where(picked, tail, 0.0), axis=-1, keepdims=True)
    pieces, wide = ys.shape[0], ys.shape[-1]

    def pass_on(n):
        whole(y_in.at[n], ra.at[n]).wait_recv()
        for q in range(1, zs):
            ys[n, 0, across, q] = (
                ys[n, 0, across, q].astype(f32) + y_in[n, across, q].astype(f32)
            ).astype(bf16)
            send(ys.at[n, 0, across, q], dg_in.at[n, q - 1], sg, rg.at[n], far_z(-q))
        for d in (1, 2):
            ys[n, 0, d] = (ys[n, 0, d].astype(f32) + y_in[n, d].astype(f32)).astype(bf16)
            send(ys.at[n, 0, d], z_in.at[n, d - 1], sb, rb.at[n], far_lane(d))

    for n in range(pieces):
        cols = slice(n * wide, (n + 1) * wide)
        made = jnp.dot(hid[...], ed[:, cols], preferred_element_type=f32) * scale
        for d in range(lanes):
            piece = made[d * block : (d + 1) * block]
            if d == 0:
                piece = piece + dens[:, cols]
            ys[n, :, d] = piece.reshape(2, zs, rows, wide).astype(bf16)
        send(ys.at[n, 1], y_in.at[n], sa, ra.at[n], partner)
        if n > 0:
            pass_on(n - 1)
    pass_on(pieces - 1)
    for n in range(pieces):
        cols = slice(n * wide, (n + 1) * wide)
        total = ys[n, 0, across, 0].astype(f32) + y_in[n, across, 0].astype(f32)
        whole(dg_in.at[n], rg.at[n]).wait_recv()
        for q in range(1, zs):
            total = total + dg_in[n, q - 1].astype(f32)
        d_out[n] = total.astype(bf16)
        send(d_out.at[n], d_in.at[n], sd, rd.at[n], far_lane(across))
        total = ys[n, 0, 0].astype(f32) + y_in[n, 0].astype(f32)
        whole(z_in.at[n], rb.at[n]).wait_recv()
        for d in (1, 2):
            total = total + z_in[n, d - 1].astype(f32)
        v_out[n] = total.astype(bf16)
        for q in range(1, zs):
            send(v_out.at[n, q], v_in.at[n, q - 1], sv, rv.at[n], far_z(-q))
        hid_rows[:, cols] = hid_rows[:, cols] + total[0]
    whole(p_in, s1).wait_send()
    whole(xs.at[:, 1:, 0], st.at[0]).wait_send()
    whole(xs.at[0, 1:, 1:], st.at[1]).wait_send()
    whole(xs.at[1], sc).wait_send()
    whole(y_in, sa).wait_send()
    whole(dg_in, sg).wait_send()
    whole(z_in, sb).wait_send()
    for n in range(pieces):
        cols = slice(n * wide, (n + 1) * wide)
        result = hid_rows[:, cols]
        whole(d_in.at[n], rd.at[n]).wait_recv()
        whole(v_in.at[n], rv.at[n]).wait_recv()
        result = result + d_in[n].astype(f32)
        for q in range(1, zs):
            result = result + v_in[n, q - 1].astype(f32)
        out_ref[:, cols] = result.astype(bf16)
    whole(v_in, sv).wait_send()
    whole(d_in, sd).wait_send()


def hand_over_kernel(rows_ref, state_ref, out_ref, next_ref, row_sem, state_sem):
    heads = state_ref.shape[0]
    copies = [pltpu.make_async_copy(rows_ref, out_ref, row_sem)] + [
        pltpu.make_async_copy(state_ref.at[h], next_ref.at[:, h, :], state_sem.at[h])
        for h in range(heads)
    ]
    for copy in copies:
        copy.start()
    for copy in copies:
        copy.wait()


def fused(
    tokens, recurrent_head_state, first_norm_gain, receptance_matrix, key_matrix, value_matrix,
    decay_matrix, decay_offset, correction_offset, correction_key_factor, own_term_weight,
    head_norm_gain, output_matrix, second_norm_gain, routing, routing_weight, expert_gate_weight,
    expert_up_weight, expert_down_weight, dense_gate_weight, dense_up_weight, dense_down_weight,
    dense_gate_offset,
):
    f32, bf16 = jnp.float32, jnp.bfloat16
    seqs, width = tokens.shape
    heads, flat_width = recurrent_head_state.shape[1:]
    groups, lanes = lax.axis_size("ep"), lax.axis_size("tp")
    rows, zs = seqs // lanes, groups // 2
    grant = VMEM_BYTES - rows * width * 2 - heads * seqs * flat_width * 4
    vmem = pl.BlockSpec(memory_space=pltpu.VMEM)
    anywhere = pl.BlockSpec(memory_space=pltpu.HBM)
    dma = pltpu.SemaphoreType.DMA

    def row(vector):
        return vector.reshape(1, -1)

    operands = (
        tokens, row(first_norm_gain), row(decay_offset), row(correction_offset),
        row(correction_key_factor), row(own_term_weight), row(head_norm_gain), routing.T,
        routing_weight.T, key_matrix, decay_matrix, receptance_matrix, value_matrix, output_matrix,
    )
    count = len(operands)
    hidden_units = expert_gate_weight.shape[2]
    pieces = 4
    wide = width // pieces
    total = groups * seqs
    pair = 2 * HEAD_WIDTH
    next_state, layer_rows = pl.pallas_call(
        functools.partial(fused_kernel, count, groups, lanes),
        out_shape=(
            pltpu.VMEM((heads, seqs, flat_width), f32),
            pltpu.VMEM((rows, width), bf16),
        ),
        in_specs=[anywhere] * (count + 9),
        out_specs=(vmem, vmem),
        scratch_shapes=[pltpu.VMEM(operand.shape, operand.dtype) for operand in operands]
        + [
            pltpu.VMEM((heads, seqs, flat_width), f32),
            pltpu.VMEM((2 * heads * seqs, flat_width), bf16),
            pltpu.VMEM((flat_width, pair), bf16),
            pltpu.VMEM((pair, flat_width), bf16),
            pltpu.VMEM((2 * heads * seqs, pair), bf16),
            pltpu.VMEM(expert_gate_weight.shape[1:], bf16),
            pltpu.VMEM(expert_up_weight.shape[1:], bf16),
            pltpu.VMEM(expert_down_weight.shape[1:], bf16),
            pltpu.VMEM(dense_gate_weight.shape[::-1], bf16),
            pltpu.VMEM(dense_up_weight.shape[::-1], bf16),
            pltpu.VMEM(dense_down_weight.shape, bf16),
            pltpu.VMEM((1, width), f32),
            pltpu.VMEM((1, width), f32),
            pltpu.VMEM((lanes, rows, width), bf16),
            pltpu.VMEM((rows, width), f32),
            pltpu.VMEM((lanes - 1, rows, width), bf16),
            pltpu.VMEM((2, lanes, zs, rows, width + 128), bf16),
            pltpu.VMEM((total, width + 128), bf16),
            pltpu.VMEM((total, hidden_units), bf16),
            pltpu.VMEM((2 * zs * rows, width), f32),
            pltpu.VMEM((pieces, 2, lanes, zs, rows, wide), bf16),
            pltpu.VMEM((pieces, lanes, zs, rows, wide), bf16),
            pltpu.VMEM((pieces, 2, zs, rows, wide), bf16),
            pltpu.VMEM((pieces, zs, rows, wide), bf16),
            pltpu.VMEM((pieces, zs - 1, rows, wide), bf16),
            pltpu.VMEM((pieces, zs - 1, rows, wide), bf16),
            pltpu.VMEM((pieces, rows, wide), bf16),
            pltpu.VMEM((pieces, rows, wide), bf16),
            dma((count,)),
            dma((heads,)),
            dma((8,)),
            dma, dma, dma((2,)), dma((lanes * zs,)), dma, dma((2,)),
            dma, dma((pieces,)), dma, dma((pieces,)), dma, dma((pieces,)),
            dma, dma((pieces,)), dma, dma((pieces,)),
        ],
        compiler_params=pltpu.CompilerParams(
            collective_id=0, has_side_effects=True, vmem_limit_bytes=grant
        ),
        name="layer",
    )(
        *operands, recurrent_head_state, row(second_norm_gain), row(dense_gate_offset),
        expert_gate_weight, expert_up_weight, expert_down_weight, dense_gate_weight.T,
        dense_up_weight.T, dense_down_weight,
    )
    return pl.pallas_call(
        hand_over_kernel,
        out_shape=(
            jax.ShapeDtypeStruct((rows, width), bf16),
            jax.ShapeDtypeStruct(recurrent_head_state.shape, f32),
        ),
        in_specs=[vmem, vmem],
        out_specs=(anywhere, anywhere),
        scratch_shapes=[dma, dma((heads,))],
        compiler_params=pltpu.CompilerParams(vmem_limit_bytes=1 << 20),
        name="hand_over",
    )(
        pltpu.with_memory_space_constraint(layer_rows, pltpu.VMEM),
        pltpu.with_memory_space_constraint(next_state, pltpu.VMEM),
    )


def choose(tokens, recurrent_head_state, *rest):
    groups, lanes = lax.axis_size("ep"), lax.axis_size("tp")
    rows, heads = tokens.shape[0] // lanes, recurrent_head_state.shape[1]
    experts_here = rest[14].shape[0]
    fits = (
        rows % 8 == 0 and heads % 2 == 0 and groups % 2 == 0 and groups > 2 and lanes == 4
        and groups <= 64 and experts_here == 1
    )
    return (fused if fits else local)(tokens, recurrent_head_state, *rest)


def solution(mesh):
    return jax.shard_map(
        choose,
        mesh=mesh,
        in_specs=(
            P("ep", None),
            P("ep", "tp", None),
            P(),
            P(None, "tp"),
            P(None, "tp"),
            P(None, "tp"),
            P(None, "tp"),
            P("tp"),
            P("tp"),
            P("tp"),
            P("tp"),
            P("tp"),
            P("tp", None),
            P(),
            P(),
            P("ep", None),
            P("ep", None, "tp"),
            P("ep", None, "tp"),
            P("ep", "tp", None),
            P(None, "ep"),
            P(None, "ep"),
            P("ep", None),
            P(),
        ),
        out_specs=(P(("ep", "tp"), None), P("ep", "tp", None)),
        check_vma=False,
    )
```

```python
import functools

import jax
import jax.numpy as jnp
from jax import lax
from jax.experimental import pallas as pl
from jax.experimental.pallas import tpu as pltpu
from jax.sharding import PartitionSpec as P

HEAD_WIDTH = 64
VMEM_BYTES = 67043328


PRECISE = lax.Precision.HIGHEST


def rms_scale(rows, gain):
    floats = rows.astype(jnp.float32)
    return floats * lax.rsqrt(jnp.mean(floats * floats, axis=-1, keepdims=True) + 1e-06) * gain


def route_table(block_routes, experts, capacity):
    flat_routes = block_routes.reshape(-1)
    chosen = (flat_routes[:, None] == jnp.arange(experts, dtype=jnp.int32)[None, :]).astype(
        jnp.int32
    )
    before = jnp.cumsum(chosen, axis=0, dtype=jnp.int32) - chosen
    slot_index = jnp.sum(before * chosen, axis=1)
    slot_match = (slot_index[:, None] == jnp.arange(capacity, dtype=jnp.int32)[None, :]).astype(
        jnp.float32
    )
    dispatch_table = chosen.astype(jnp.float32)[:, :, None] * slot_match[:, None, :]
    return dispatch_table.reshape(block_routes.shape[0], block_routes.shape[1], experts, capacity)


def state_update(
    receptance_rows,
    key_matrix_rows,
    value_matrix_rows,
    decay_logits,
    recurrent_head_state,
    decay_offset,
    correction_offset,
    correction_key_factor,
    own_term_weight,
    head_norm_gain,
    head_width,
):
    seq_count = key_matrix_rows.shape[0]
    decay_factor = jnp.exp(-jnp.exp(decay_offset + decay_logits))
    in_rate = jax.nn.sigmoid(correction_offset + correction_key_factor * key_matrix_rows)
    key_in = key_matrix_rows * in_rate

    def split_heads(block):
        return block.reshape(seq_count, -1, head_width)

    keys_head = split_heads(key_matrix_rows)
    unit_keys = (
        keys_head
        * lax.rsqrt(jnp.mean(keys_head * keys_head, axis=-1, keepdims=True) + 1e-06)
        * head_width ** (-0.5)
    )
    rate_head = split_heads(in_rate)
    head_keys = split_heads(key_in)
    decay_head = split_heads(decay_factor)
    head_values = split_heads(value_matrix_rows)
    head_receptance = split_heads(receptance_rows)
    matrix = recurrent_head_state.reshape(seq_count, -1, head_width, head_width)
    removed = jnp.einsum("bhvk,bhk->bhv", matrix, unit_keys, precision=PRECISE)
    updated = (
        matrix * decay_head[:, :, None, :]
        - removed[..., None] * (unit_keys * rate_head)[:, :, None, :]
        + head_values[..., None] * head_keys[:, :, None, :]
    )
    readout = jnp.einsum("bhvk,bhk->bhv", updated, head_receptance, precision=PRECISE)
    center = jnp.mean(readout, axis=-1, keepdims=True)
    spread = jnp.mean(jnp.square(readout - center), axis=-1, keepdims=True)
    normalized_rows = (
        (readout - center) * lax.rsqrt(spread + 0.00064) * head_norm_gain.reshape(-1, head_width)
    )
    own_term_total = jnp.sum(
        head_receptance * head_keys * own_term_weight.reshape(-1, head_width),
        axis=-1,
        keepdims=True,
    )
    normalized_rows = normalized_rows + own_term_total * head_values
    return (
        normalized_rows.reshape(seq_count, -1).astype(jnp.bfloat16),
        updated.reshape(seq_count, -1, head_width * head_width),
    )


def local(
    tokens,
    recurrent_head_state,
    first_norm_gain,
    receptance_matrix,
    key_matrix,
    value_matrix,
    decay_matrix,
    decay_offset,
    correction_offset,
    correction_key_factor,
    own_term_weight,
    head_norm_gain,
    output_matrix,
    second_norm_gain,
    routing,
    routing_weight,
    expert_gate_weight,
    expert_up_weight,
    expert_down_weight,
    dense_gate_weight,
    dense_up_weight,
    dense_down_weight,
    dense_gate_offset,
):
    seq_count = tokens.shape[0]
    width = tokens.shape[1]
    group_index = lax.axis_index("ep")
    lane_index = lax.axis_index("tp")
    group_count = lax.axis_size("ep")
    lane_count = lax.axis_size("tp")
    normalized_rows = rms_scale(tokens, first_norm_gain).astype(jnp.bfloat16)
    receptance_rows = jnp.dot(
        normalized_rows, receptance_matrix, preferred_element_type=jnp.float32
    )
    key_matrix_rows = jnp.dot(normalized_rows, key_matrix, preferred_element_type=jnp.float32)
    value_matrix_rows = jnp.dot(normalized_rows, value_matrix, preferred_element_type=jnp.float32)
    decay_logits = jnp.dot(normalized_rows, decay_matrix, preferred_element_type=jnp.float32)
    head_outputs, next_state = state_update(
        receptance_rows,
        key_matrix_rows,
        value_matrix_rows,
        decay_logits,
        recurrent_head_state,
        decay_offset,
        correction_offset,
        correction_key_factor,
        own_term_weight,
        head_norm_gain,
        HEAD_WIDTH,
    )
    partial_out = jnp.dot(head_outputs, output_matrix, preferred_element_type=jnp.float32)
    hidden_sum = tokens.astype(jnp.float32) + lax.psum(
        partial_out.astype(jnp.bfloat16), "tp"
    ).astype(jnp.float32)
    ffn_in = rms_scale(hidden_sum, second_norm_gain).astype(jnp.bfloat16)
    local_experts = expert_gate_weight.shape[0]
    top_count = routing.shape[1]
    expert_count = local_experts * group_count
    capacity = 2 * seq_count * top_count // expert_count
    per_lane = seq_count // lane_count
    own_routes = lax.dynamic_slice_in_dim(routing, group_index * seq_count, seq_count, 0)
    own_table = route_table(own_routes, expert_count, capacity)
    send_rows = jnp.einsum(
        "bkec,bd->ecd", own_table.astype(jnp.bfloat16), ffn_in, preferred_element_type=jnp.float32
    ).astype(jnp.bfloat16)
    lane_rows = lax.dynamic_slice_in_dim(ffn_in, lane_index * per_lane, per_lane, 0)
    dense_send = jnp.broadcast_to(lane_rows[None], (group_count, per_lane, width))
    expert_in, dense_in = (
        lax.all_to_all(send_rows, "ep", split_axis=0, concat_axis=0, tiled=True),
        lax.all_to_all(dense_send, "ep", split_axis=0, concat_axis=0, tiled=True),
    )
    rows_in = expert_in.reshape(group_count, local_experts, capacity, width).transpose(1, 0, 2, 3)
    rows_in = rows_in.reshape(local_experts, group_count * capacity, width)
    gate_pre = jnp.einsum(
        "lrd,ldf->lrf", rows_in, expert_gate_weight, preferred_element_type=jnp.float32
    )
    up_pre = jnp.einsum(
        "lrd,ldf->lrf", rows_in, expert_up_weight, preferred_element_type=jnp.float32
    )
    expert_hidden = (jax.nn.silu(gate_pre) * up_pre).astype(jnp.bfloat16)
    expert_part = jnp.einsum(
        "lrf,lfd->lrd", expert_hidden, expert_down_weight, preferred_element_type=jnp.float32
    )
    expert_out = lax.psum_scatter(
        expert_part.astype(jnp.bfloat16), "tp", scatter_dimension=2, tiled=True
    )
    back_send = expert_out.reshape(local_experts, group_count, capacity, -1).transpose(1, 0, 2, 3)
    back_send = back_send.reshape(group_count * local_experts, capacity, -1)
    dense_rows = dense_in.reshape(group_count * per_lane, width)
    dense_hidden = (
        jax.nn.silu(jnp.dot(dense_rows, dense_gate_weight, preferred_element_type=jnp.float32))
        * jnp.dot(dense_rows, dense_up_weight, preferred_element_type=jnp.float32)
    ).astype(jnp.bfloat16)
    dense_part = jnp.dot(
        dense_hidden, dense_down_weight, preferred_element_type=jnp.float32
    ).astype(jnp.bfloat16)
    dense_part = dense_part.reshape(group_count, per_lane, width)
    back_experts, back_dense = (
        lax.all_to_all(back_send, "ep", split_axis=0, concat_axis=0, tiled=True),
        lax.all_to_all(dense_part, "ep", split_axis=0, concat_axis=0, tiled=True),
    )
    dense_sum = jnp.sum(back_dense.astype(jnp.float32), axis=0)
    weighted = jnp.einsum("bkec,bk->ecb", own_table, routing_weight, precision=PRECISE)
    moe_slice = jnp.einsum(
        "ecb,ecd->bd", weighted, back_experts.astype(jnp.float32), precision=PRECISE
    )
    moe_rows = lax.all_to_all(moe_slice, "tp", split_axis=0, concat_axis=1, tiled=True)
    residual_rows = lax.dynamic_slice_in_dim(hidden_sum, lane_index * per_lane, per_lane, 0)
    layer_out = (residual_rows + moe_rows + jax.nn.sigmoid(dense_gate_offset) * dense_sum).astype(
        jnp.bfloat16
    )
    return (layer_out, next_state)


def fused_kernel(count, groups, lanes, *refs):
    sources, refs = refs[:count], refs[count:]
    state_ref, gain_hbm, goff_hbm, eg_hbm, eu_hbm, ed_hbm, dg_hbm, du_hbm, dd_hbm = refs[:9]
    nbuf, out_ref = refs[9:11]
    held, refs = refs[11 : 11 + count], refs[11 + count :]
    (tokens_ref, gain_ref, doff_ref, coff_ref, cfac_ref, own_ref, hgain_ref, routes_ref,
     rweight_ref, wk_ref, wd_ref, wr_ref, wv_ref, wo_ref) = held
    (sbuf, pbuf, gather_ones, spread_ones, spread_in,
     eg, eu, ed, dg, du, dd, gain, goff, part_ref, hid_rows, p_in, xs, flat, hid, dens,
     ys, y_in, z_in, v_out, v_in, dg_in, d_out, d_in,
     arg_sem, in_sem,
     w_sem, s1, r1, st, rt, sc, rc, sa, ra, sb, rb, sv, rv, sg, rg, sd, rd) = refs
    f32, bf16 = jnp.float32, jnp.bfloat16
    zs = groups // 2
    me_g, me_l = lax.axis_index("ep"), lax.axis_index("tp")
    core, me_z = lax.rem(me_g, 2), me_g // 2
    partner = (me_g + 1 - 2 * core, me_l)

    side_x, side_y = lax.rem(me_l, 2), me_l // 2

    def lane_at(d):
        flip_x, flip_y = d % 2, d // 2
        x = side_x + flip_x - 2 * flip_x * side_x
        y = side_y + flip_y - 2 * flip_y * side_y
        return 2 * y + x

    def lane_peer(d):
        return (me_g, lane_at(d))

    def far_lane(d):
        return (partner[0], lane_at(d))

    def far_z(d):
        return (lax.rem(me_z + d + zs, zs) * 2 + 1 - core, me_l)

    def send(src, dst, ssem, rsem, peer):
        copy = pltpu.make_async_remote_copy(
            src_ref=src, dst_ref=dst, send_sem=ssem, recv_sem=rsem, device_id=peer,
            device_id_type=pl.DeviceIdType.MESH,
        )
        copy.start()
        return copy

    def whole(ref, sem):
        return pltpu.make_async_remote_copy(
            src_ref=ref, dst_ref=ref, send_sem=sem, recv_sem=sem, device_id=partner,
            device_id_type=pl.DeviceIdType.MESH,
        )

    seqs, width = tokens_ref.shape
    heads = state_ref.shape[1]
    rows = seqs // lanes
    args = [
        pltpu.make_async_copy(src, dst, arg_sem.at[i])
        for i, (src, dst) in enumerate(zip(sources, held))
    ]
    loads = [
        pltpu.make_async_copy(state_ref.at[:, h, :], sbuf.at[h], in_sem.at[h]) for h in range(heads)
    ]
    for arg in args[:-2]:
        arg.start()
    for load in loads:
        load.start()
    for arg in args[-2:]:
        arg.start()
    barrier = pltpu.get_barrier_semaphore()
    peers = [lane_peer(d) for d in range(1, lanes)] + [far_lane(d) for d in range(1, lanes)]
    peers += [far_z(d) for d in range(1, zs)] + [partner]
    for peer in peers:
        pl.semaphore_signal(barrier, inc=1, device_id=peer, device_id_type=pl.DeviceIdType.MESH)

    pair = 2 * HEAD_WIDTH
    flat_width = state_ref.shape[2]
    tile = 256

    offset = (
        lax.broadcasted_iota(jnp.int32, (tile, pair), 0) // HEAD_WIDTH
        - lax.broadcasted_iota(jnp.int32, (tile, pair), 1) % HEAD_WIDTH
    )
    for n in range(0, flat_width, tile):
        gather_ones[n : n + tile, :] = jnp.where(offset == -(n // HEAD_WIDTH), 1.0, 0.0).astype(bf16)

    half_r = lax.broadcasted_iota(jnp.int32, (pair, pair), 0) // HEAD_WIDTH
    half_c = lax.broadcasted_iota(jnp.int32, (pair, pair), 1) // HEAD_WIDTH
    ones_block = (half_r == half_c).astype(f32).astype(bf16)

    def group_sums(*blocks):
        parts = []
        for block in blocks:
            for i in range(0, block.shape[1], pair):
                piece = block[:, i : i + pair]
                high = piece.astype(bf16)
                parts += [high, (piece - high.astype(f32)).astype(bf16)]
        made = jnp.dot(jnp.concatenate(parts, axis=0), ones_block, preferred_element_type=f32)
        sums, at = [], 0
        for block in blocks:
            cols = []
            for i in range(0, block.shape[1], pair):
                cols.append(made[at : at + seqs] + made[at + seqs : at + 2 * seqs])
                at += 2 * seqs
            sums.append(jnp.concatenate(cols, axis=1))
        return sums

    lane = lax.broadcasted_iota(jnp.int32, (seqs, pair), 1)
    low = lane < HEAD_WIDTH

    def doubled(full, h):
        chunk = full[:, (h // 2) * pair : (h // 2 + 1) * pair]
        turned = pltpu.roll(chunk, HEAD_WIDTH, 1)
        return jnp.where(low, chunk, turned) if h % 2 == 0 else jnp.where(low, turned, chunk)

    for arg in args[:9]:
        arg.wait()
    toks = tokens_ref[...].astype(f32)
    normed = (
        toks * lax.rsqrt(jnp.mean(toks * toks, axis=-1, keepdims=True) + 1e-06) * gain_ref[...]
    ).astype(bf16)
    start = me_g * seqs + me_l * rows

    def picked_column(ref, k, first):
        spot = lax.broadcasted_iota(jnp.int32, (rows, ref.shape[1]), 1)
        wanted = spot == first + lax.broadcasted_iota(jnp.int32, spot.shape, 0)
        entries = ref[k : k + 1, :].astype(f32)
        return jnp.sum(jnp.where(wanted, entries, 0.0), axis=-1, keepdims=True)

    column = lax.broadcasted_iota(jnp.int32, (rows, 128), 1) % 64
    column = column.astype(f32)
    table = jnp.zeros((rows, 128), f32)
    for k in range(routes_ref.shape[0]):
        expert = picked_column(routes_ref, k, start)
        table = table + jnp.where(
            column == expert, picked_column(rweight_ref, k, me_l * rows), 0.0
        )
    high = table.astype(bf16).astype(f32)
    first_half = lax.broadcasted_iota(jnp.int32, table.shape, 1) < 64
    xs[0, 0, 0, :, width:] = jnp.where(first_half, high, table - high).astype(bf16)

    args[9].wait()
    keys = jnp.dot(normed, wk_ref[...], preferred_element_type=f32)
    args[10].wait()
    logits = jnp.dot(normed, wd_ref[...], preferred_element_type=f32)
    args[11].wait()
    recept = jnp.dot(normed, wr_ref[...], preferred_element_type=f32)
    for load in loads:
        load.wait()
    args[12].wait()
    values = jnp.dot(normed, wv_ref[...], preferred_element_type=f32)
    pulls = [
        pltpu.make_async_copy(src, dst, w_sem.at[i])
        for i, (src, dst) in enumerate(
            [(gain_hbm, gain), (goff_hbm, goff), (dg_hbm, dg), (du_hbm, du), (dd_hbm, dd),
             (eg_hbm.at[0], eg), (eu_hbm.at[0], eu), (ed_hbm.at[0], ed)]
        )
    ]
    for pull in pulls:
        pull.start()

    (key_squares,) = group_sums(keys * keys)
    rate = jax.nn.sigmoid(coff_ref[...] + cfac_ref[...] * keys)
    unit = keys * lax.rsqrt(key_squares * (1.0 / HEAD_WIDTH) + 1e-06) * HEAD_WIDTH ** (-0.5)
    key_in = keys * rate
    back = unit * rate
    decay = jnp.exp(-jnp.exp(doff_ref[...] + logits))
    faded = decay * recept
    back_sum, in_sum, own_sum = group_sums(
        back * recept, key_in * recept, recept * key_in * own_ref[...]
    )
    for h in range(heads):
        u2, f2 = doubled(unit, h), doubled(faded, h)
        for j in range(0, flat_width, pair):
            old = sbuf[h, :, j : j + pair]
            pbuf[2 * h * seqs : (2 * h + 1) * seqs, j : j + pair] = (old * u2).astype(bf16)
            pbuf[(2 * h + 1) * seqs : (2 * h + 2) * seqs, j : j + pair] = (old * f2).astype(bf16)
    sums = jnp.dot(pbuf[...], gather_ones[...], preferred_element_type=f32)

    def merged(first):
        picks = [sums[(2 * h + first) * seqs : (2 * h + first + 1) * seqs] for h in range(heads)]
        return jnp.concatenate(
            [jnp.where(low, picks[h], picks[h + 1]) for h in range(0, heads, 2)], axis=1
        )

    read = merged(1) - merged(0) * back_sum + values * in_sum
    (read_sum,) = group_sums(read)
    center = read - read_sum * (1.0 / HEAD_WIDTH)
    (square_sum,) = group_sums(center * center)
    heads_out = (
        center * lax.rsqrt(square_sum * (1.0 / HEAD_WIDTH) + 0.00064) * hgain_ref[...]
        + own_sum * values
    ).astype(bf16)
    args[13].wait()
    part = jnp.dot(heads_out, wo_ref[...], preferred_element_type=f32)
    base = jnp.zeros((rows, width), f32)
    for i in range(lanes):
        mine = part[i * rows : (i + 1) * rows]
        part_ref[i] = mine.astype(bf16)
        base = jnp.where(me_l == i, mine + toks[i * rows : (i + 1) * rows], base)
    hid_rows[...] = base
    pl.semaphore_wait(barrier, len(peers))
    across = lanes - 1
    for d in (across, 1, 2):
        send(part_ref.at[lane_at(d)], p_in.at[d - 1], s1, r1, lane_peer(d))
    offset = (
        lax.broadcasted_iota(jnp.int32, (pair, tile), 0) % HEAD_WIDTH
        - lax.broadcasted_iota(jnp.int32, (pair, tile), 1) // HEAD_WIDTH
    )
    for n in range(0, flat_width, tile):
        spread_ones[:, n : n + tile] = jnp.where(offset == n // HEAD_WIDTH, 1.0, 0.0).astype(bf16)

    def halves(block):
        high = block.astype(bf16).astype(f32)
        return jnp.where(low, high, block - high).astype(bf16)

    for h in range(heads):
        spread_in[2 * h * seqs : (2 * h + 1) * seqs] = halves(
            sums[2 * h * seqs : (2 * h + 1) * seqs]
        )
        spread_in[(2 * h + 1) * seqs : (2 * h + 2) * seqs] = halves(doubled(values, h))
    fades = [doubled(decay, h) for h in range(heads)]
    backs = [doubled(back, h) for h in range(heads)]
    ins = [doubled(key_in, h) for h in range(heads)]
    for n in range(0, flat_width, tile):
        wide_rows = jnp.dot(
            spread_in[...], spread_ones[:, n : n + tile], preferred_element_type=f32
        )
        for h in range(heads):
            gone = wide_rows[2 * h * seqs : (2 * h + 1) * seqs]
            came = wide_rows[(2 * h + 1) * seqs : (2 * h + 2) * seqs]
            for i in range(0, tile, pair):
                nbuf[h, :, n + i : n + i + pair] = (
                    sbuf[h, :, n + i : n + i + pair] * fades[h]
                    - gone[:, i : i + pair] * backs[h]
                    + came[:, i : i + pair] * ins[h]
                )
    hidden = hid_rows[...]
    whole(p_in, r1).wait_recv()
    for d in range(1, lanes):
        hidden = hidden + p_in[d - 1].astype(f32)
    hid_rows[...] = hidden
    for pull in pulls[:2]:
        pull.wait()
    normed = hidden * lax.rsqrt(jnp.mean(hidden * hidden, axis=-1, keepdims=True) + 1e-06)
    xs[0, 0, 0, :, :width] = (normed * gain[...]).astype(bf16)
    hold = {}

    def pass_block(d, q, to_d, to_q, peer):
        hold[to_d, to_q] = send(
            xs.at[0, d, q], xs.at[0, to_d, to_q], st.at[0 if (d, q) == (0, 0) else 1],
            rt.at[to_d * zs + to_q], peer,
        )

    def to_partner(d, q):
        send(xs.at[0, d, q], xs.at[1, d, q], sc, rc.at[0 if d == 0 else 1], partner)

    pass_block(0, 0, across, 0, far_lane(across))
    for q in range(1, zs):
        pass_block(0, 0, 0, q, far_z(q))
    for d in (1, 2):
        pass_block(0, 0, d, 0, far_lane(d))
    to_partner(0, 0)

    def spread_row(q):
        hold[0, q].wait_recv()
        for d in (1, 2):
            pass_block(0, q, d, q, far_lane(d))
        to_partner(0, q)

    hold[across, 0].wait_recv()
    for q in range(1, zs):
        pass_block(across, 0, across, q, far_z(q))
    for q in range(zs - 1, 0, -1):
        spread_row(q)
    to_partner(across, 0)
    for d in (1, 2):
        hold[d, 0].wait_recv()
        to_partner(d, 0)
    block = 2 * zs * rows

    def gathered(d):
        return xs[:, d].astype(f32).reshape(block, width + 128)

    whole(xs.at[1, 0], rc.at[0]).wait_recv()
    mine = gathered(0)
    flat[0:block] = mine.astype(bf16)
    own_rows = mine[:, :width].astype(bf16)
    for pull in pulls[2:5]:
        pull.wait()
    turned = (((1,), (1,)), ((), ()))
    gate = lax.dot_general(own_rows, dg[...], turned, preferred_element_type=f32)
    up = lax.dot_general(own_rows, du[...], turned, preferred_element_type=f32)
    mixed = (jax.nn.silu(gate) * up).astype(bf16)
    dens[...] = jnp.dot(mixed, dd[...], preferred_element_type=f32) * jax.nn.sigmoid(goff[...])
    for q in range(zs - 1, 0, -1):
        for d in range(1, lanes):
            hold[d, q].wait_recv()
            to_partner(d, q)
    whole(xs.at[1, 1:], rc.at[1]).wait_recv()
    for d in range(1, lanes):
        flat[d * block : (d + 1) * block] = gathered(d).astype(bf16)
    for pull in pulls[5:]:
        pull.wait()

    @pl.loop(0, eg.shape[1] // tile, unroll=True)
    def _(n):
        cols = pl.ds(pl.multiple_of(n * tile, tile), tile)
        left = flat[:, :width]
        gated = jnp.dot(left, eg[:, cols], preferred_element_type=f32)
        raised = jnp.dot(left, eu[:, cols], preferred_element_type=f32)
        hid[:, cols] = (jax.nn.silu(gated) * raised).astype(bf16)

    tail = flat[:, width:].astype(f32)
    picked = lax.broadcasted_iota(jnp.int32, tail.shape, 1) % 64 == me_g
    scale = jnp.sum(jnp.where(picked, tail, 0.0), axis=-1, keepdims=True)
    pieces = 4
    edges = [n * (width // pieces) for n in range(pieces + 1)]
    spans = [slice(low_edge, high_edge) for low_edge, high_edge in zip(edges, edges[1:])]

    def pass_on(n):
        cols = spans[n]
        whole(y_in.at[:, :, :, cols], ra.at[n]).wait_recv()
        for q in range(1, zs):
            ys[0, across, q, :, cols] = (
                ys[0, across, q, :, cols].astype(f32) + y_in[across, q, :, cols].astype(f32)
            ).astype(bf16)
            send(ys.at[0, across, q, :, cols], dg_in.at[q - 1, :, cols], sg, rg.at[n], far_z(-q))
        for d in (1, 2):
            ys[0, d, :, :, cols] = (ys[0, d, :, :, cols].astype(f32) + y_in[d, :, :, cols].astype(f32)).astype(bf16)
            send(ys.at[0, d, :, :, cols], z_in.at[d - 1, :, :, cols], sb, rb.at[n], far_lane(d))

    for n in range(pieces):
        cols = spans[n]
        wide = cols.stop - cols.start
        made = jnp.dot(hid[...], ed[:, cols], preferred_element_type=f32) * scale
        for d in range(lanes):
            piece = made[d * block : (d + 1) * block]
            if d == 0:
                piece = piece + dens[:, cols]
            ys[:, d, :, :, cols] = piece.reshape(2, zs, rows, wide).astype(bf16)
        send(ys.at[1, :, :, :, cols], y_in.at[:, :, :, cols], sa, ra.at[n], partner)
        if n > 0:
            pass_on(n - 1)
    pass_on(pieces - 1)
    for n in range(pieces):
        cols = spans[n]
        wide = cols.stop - cols.start
        total = ys[0, 0, :, :, cols].astype(f32) + y_in[0, :, :, cols].astype(f32)
        whole(z_in.at[:, :, :, cols], rb.at[n]).wait_recv()
        for d in (1, 2):
            total = total + z_in[d - 1, :, :, cols].astype(f32)
        v_out[:, :, cols] = total.astype(bf16)
        for q in range(1, zs):
            send(v_out.at[q, :, cols], v_in.at[q - 1, :, cols], sv, rv.at[n], far_z(-q))
        hid_rows[:, cols] = hid_rows[:, cols] + total[0]
        total = ys[0, across, 0, :, cols].astype(f32) + y_in[across, 0, :, cols].astype(f32)
        whole(dg_in.at[:, :, cols], rg.at[n]).wait_recv()
        for q in range(1, zs):
            total = total + dg_in[q - 1, :, cols].astype(f32)
        d_out[:, cols] = total.astype(bf16)
        send(d_out.at[:, cols], d_in.at[:, cols], sd, rd.at[n], far_lane(across))
    whole(p_in, s1).wait_send()
    whole(xs.at[:, 1:, 0], st.at[0]).wait_send()
    whole(xs.at[0, 1:, 1:], st.at[1]).wait_send()
    whole(xs.at[1], sc).wait_send()
    whole(y_in, sa).wait_send()
    whole(dg_in, sg).wait_send()
    whole(z_in, sb).wait_send()
    for n in range(pieces):
        cols = spans[n]
        wide = cols.stop - cols.start
        result = hid_rows[:, cols]
        whole(d_in.at[:, cols], rd.at[n]).wait_recv()
        whole(v_in.at[:, :, cols], rv.at[n]).wait_recv()
        result = result + d_in[:, cols].astype(f32)
        for q in range(1, zs):
            result = result + v_in[q - 1, :, cols].astype(f32)
        out_ref[:, cols] = result.astype(bf16)
    whole(v_in, sv).wait_send()
    whole(d_in, sd).wait_send()


def hand_over_kernel(rows_ref, state_ref, out_ref, next_ref, row_sem, state_sem):
    heads = state_ref.shape[0]
    copies = [pltpu.make_async_copy(rows_ref, out_ref, row_sem)] + [
        pltpu.make_async_copy(state_ref.at[h], next_ref.at[:, h, :], state_sem.at[h])
        for h in range(heads)
    ]
    for copy in copies:
        copy.start()
    for copy in copies:
        copy.wait()


def fused(
    tokens, recurrent_head_state, first_norm_gain, receptance_matrix, key_matrix, value_matrix,
    decay_matrix, decay_offset, correction_offset, correction_key_factor, own_term_weight,
    head_norm_gain, output_matrix, second_norm_gain, routing, routing_weight, expert_gate_weight,
    expert_up_weight, expert_down_weight, dense_gate_weight, dense_up_weight, dense_down_weight,
    dense_gate_offset,
):
    f32, bf16 = jnp.float32, jnp.bfloat16
    seqs, width = tokens.shape
    heads, flat_width = recurrent_head_state.shape[1:]
    groups, lanes = lax.axis_size("ep"), lax.axis_size("tp")
    rows, zs = seqs // lanes, groups // 2
    grant = VMEM_BYTES - rows * width * 2 - heads * seqs * flat_width * 4
    vmem = pl.BlockSpec(memory_space=pltpu.VMEM)
    anywhere = pl.BlockSpec(memory_space=pltpu.HBM)
    dma = pltpu.SemaphoreType.DMA

    def row(vector):
        return vector.reshape(1, -1)

    operands = (
        tokens, row(first_norm_gain), row(decay_offset), row(correction_offset),
        row(correction_key_factor), row(own_term_weight), row(head_norm_gain), routing.T,
        routing_weight.T, key_matrix, decay_matrix, receptance_matrix, value_matrix, output_matrix,
    )
    count = len(operands)
    hidden_units = expert_gate_weight.shape[2]
    pieces = 4
    total = groups * seqs
    pair = 2 * HEAD_WIDTH
    next_state, layer_rows = pl.pallas_call(
        functools.partial(fused_kernel, count, groups, lanes),
        out_shape=(
            pltpu.VMEM((heads, seqs, flat_width), f32),
            pltpu.VMEM((rows, width), bf16),
        ),
        in_specs=[anywhere] * (count + 9),
        out_specs=(vmem, vmem),
        scratch_shapes=[pltpu.VMEM(operand.shape, operand.dtype) for operand in operands]
        + [
            pltpu.VMEM((heads, seqs, flat_width), f32),
            pltpu.VMEM((2 * heads * seqs, flat_width), bf16),
            pltpu.VMEM((flat_width, pair), bf16),
            pltpu.VMEM((pair, flat_width), bf16),
            pltpu.VMEM((2 * heads * seqs, pair), bf16),
            pltpu.VMEM(expert_gate_weight.shape[1:], bf16),
            pltpu.VMEM(expert_up_weight.shape[1:], bf16),
            pltpu.VMEM(expert_down_weight.shape[1:], bf16),
            pltpu.VMEM(dense_gate_weight.shape[::-1], bf16),
            pltpu.VMEM(dense_up_weight.shape[::-1], bf16),
            pltpu.VMEM(dense_down_weight.shape, bf16),
            pltpu.VMEM((1, width), f32),
            pltpu.VMEM((1, width), f32),
            pltpu.VMEM((lanes, rows, width), bf16),
            pltpu.VMEM((rows, width), f32),
            pltpu.VMEM((lanes - 1, rows, width), bf16),
            pltpu.VMEM((2, lanes, zs, rows, width + 128), bf16),
            pltpu.VMEM((total, width + 128), bf16),
            pltpu.VMEM((total, hidden_units), bf16),
            pltpu.VMEM((2 * zs * rows, width), f32),
            pltpu.VMEM((2, lanes, zs, rows, width), bf16),
            pltpu.VMEM((lanes, zs, rows, width), bf16),
            pltpu.VMEM((2, zs, rows, width), bf16),
            pltpu.VMEM((zs, rows, width), bf16),
            pltpu.VMEM((zs - 1, rows, width), bf16),
            pltpu.VMEM((zs - 1, rows, width), bf16),
            pltpu.VMEM((rows, width), bf16),
            pltpu.VMEM((rows, width), bf16),
            dma((count,)),
            dma((heads,)),
            dma((8,)),
            dma, dma, dma((2,)), dma((lanes * zs,)), dma, dma((2,)),
            dma, dma((pieces,)), dma, dma((pieces,)), dma, dma((pieces,)),
            dma, dma((pieces,)), dma, dma((pieces,)),
        ],
        compiler_params=pltpu.CompilerParams(
            collective_id=0, has_side_effects=True, vmem_limit_bytes=grant
        ),
        name="layer",
    )(
        *operands, recurrent_head_state, row(second_norm_gain), row(dense_gate_offset),
        expert_gate_weight, expert_up_weight, expert_down_weight, dense_gate_weight.T,
        dense_up_weight.T, dense_down_weight,
    )
    return pl.pallas_call(
        hand_over_kernel,
        out_shape=(
            jax.ShapeDtypeStruct((rows, width), bf16),
            jax.ShapeDtypeStruct(recurrent_head_state.shape, f32),
        ),
        in_specs=[vmem, vmem],
        out_specs=(anywhere, anywhere),
        scratch_shapes=[dma, dma((heads,))],
        compiler_params=pltpu.CompilerParams(vmem_limit_bytes=1 << 20),
        name="hand_over",
    )(
        pltpu.with_memory_space_constraint(layer_rows, pltpu.VMEM),
        pltpu.with_memory_space_constraint(next_state, pltpu.VMEM),
    )


def choose(tokens, recurrent_head_state, *rest):
    groups, lanes = lax.axis_size("ep"), lax.axis_size("tp")
    rows, heads = tokens.shape[0] // lanes, recurrent_head_state.shape[1]
    experts_here = rest[14].shape[0]
    fits = (
        rows % 8 == 0 and heads % 2 == 0 and groups % 2 == 0 and groups > 2 and lanes == 4
        and groups <= 64 and experts_here == 1
    )
    return (fused if fits else local)(tokens, recurrent_head_state, *rest)


def solution(mesh):
    return jax.shard_map(
        choose,
        mesh=mesh,
        in_specs=(
            P("ep", None),
            P("ep", "tp", None),
            P(),
            P(None, "tp"),
            P(None, "tp"),
            P(None, "tp"),
            P(None, "tp"),
            P("tp"),
            P("tp"),
            P("tp"),
            P("tp"),
            P("tp"),
            P("tp", None),
            P(),
            P(),
            P("ep", None),
            P("ep", None, "tp"),
            P("ep", None, "tp"),
            P("ep", "tp", None),
            P(None, "ep"),
            P(None, "ep"),
            P("ep", None),
            P(),
        ),
        out_specs=(P(("ep", "tp"), None), P("ep", "tp", None)),
        check_vma=False,
    )
```
